256 devices in a mesh: sp: 64 (over z, y, core), tp: 4 (over x).
Axes of the slice: x: 4, y: 4, z: 8, core: 2. Of those that a mesh axis runs over, the one named last changes fastest.
Arguments:
- head_queries: bfloat16 [16384, 2048], P('sp', 'tp'), may hold values from -6 to 6
- head_keys: bfloat16 [16384, 2048], P('sp', 'tp'), may hold values from -6 to 6
- head_values: bfloat16 [16384, 2048], P('sp', 'tp'), may hold values from -6 to 6
- decay_logits: bfloat16 [16384, 2048], P('sp', 'tp'), may hold values from -12 to 1
- learning_logits: bfloat16 [16384, 32], P('sp', 'tp'), may hold values from -9 to 2
- surge_decay: float32 [16384, 32], P('sp', 'tp'), may hold values from -0.7 to 0
- documents: int32 [16384], P('sp'), may hold values from 0 to 16, never falling along the last dimension, each value on 1 to 1536 neighbouring positions
- residual: bfloat16 [16384, 2048], P(('sp', 'tp')), may hold values from -6 to 6
- head_norm_scale: float32 [2048], P('tp'), may hold values from 0.1 to 1.9
- mixer_output_weight: bfloat16 [2048, 2048], P('tp'), may hold values from -0.125 to 0.125
- layer_norm_scale: float32 [2048], replicated, may hold values from 0.1 to 1.9
- routes: int32 [16384, 2], P('sp'), may hold values from 0 to 127, all different within a row; in each aligned block of 64 rows (0 to 63, 64 to 127, ...) at most 2 rows name the same one
- routing_weight: float32 [16384, 2], P(('sp', 'tp')), may hold values from 0.3 to 1.5
- routed_gate_weight: bfloat16 [128, 2048, 1024], P('sp', None, 'tp'), may hold values from -0.125 to 0.125
- routed_up_weight: bfloat16 [128, 2048, 1024], P('sp', None, 'tp'), may hold values from -0.125 to 0.125
- routed_down_weight: bfloat16 [128, 1024, 2048], P('sp', 'tp'), may hold values from -0.1875 to 0.1875
- common_gate_weight: bfloat16 [2048, 512], P(None, 'tp'), may hold values from -0.125 to 0.125
- common_up_weight: bfloat16 [2048, 512], P(None, 'tp'), may hold values from -0.125 to 0.125
- common_down_weight: bfloat16 [512, 2048], P('tp'), may hold values from -0.25 to 0.25
Outputs:
- layer_out: bfloat16 [16384, 2048], P(('sp', 'tp'))
The draws below stay inside these ranges and needn't reach their ends.
Inputs may be any that keep to these rules, and one draw needn't show every extreme that they name: `documents`: numbers never fall along the positions; each document holds 1 to 1536 positions and one holds exactly 1536. `routes`: each row names 2 different experts; in each aligned block of 64 rows no expert is named by more than 2 rows, a bound that some block reaches.
All inputs are finite; a program needn't handle non-finite values.
Results may differ from the reference program's by a relative error of at most 0.019.
Values may be sent and summed in bfloat16 or wider, within the bound.
A program may use at most 128 MiB of HBM per device.

```python
import math
import jax
import jax.numpy as jnp
import numpy as np
from jax import lax

D = 2048
HEAD_TOTAL = 32
HEAD = 64
FFE = 1024
SFF = 512
TOP = 2
TOK_DEV = 64
EXPERTS = 128
GROUP_TOK = 256
TOKEN_TOTAL = 16384
CAP = 2
DOCS = 17
DOC_MOST = 1536
SURGE_POSITIONS = 18
N_SP = 64
N_TP = 4


def slow_heads(key):
    slow_share = 0.5
    return jax.random.bernoulli(jax.random.fold_in(key, 11), slow_share, (HEAD_TOTAL,))


def draw_decay_logits(key, part):
    chosen = slow_heads(key)
    subkeys = jax.random.split(jax.random.fold_in(key, 21), 4)
    slow_level = math.log(0.3 / DOC_MOST) + 0.5
    head_level = jnp.where(chosen, slow_level, -2.95) + jax.random.uniform(subkeys[0], (HEAD_TOTAL,), jnp.float32, -0.3, 0.3)
    channel = jnp.repeat(head_level, HEAD) + jax.random.uniform(subkeys[1], (D,), jnp.float32, -0.3, 0.3)
    group_level = jnp.repeat(jax.random.uniform(subkeys[2], (TOKEN_TOTAL // GROUP_TOK,), jnp.float32, -0.4, 0.4), GROUP_TOK)
    data_part = 0.5 * jax.random.truncated_normal(subkeys[3], -4.0, 4.0, (TOKEN_TOTAL, D), jnp.float32)
    return (channel[None, :] + group_level[:, None] + data_part).astype(jnp.bfloat16)


def draw_learning_logits(key, part):
    chosen = slow_heads(key)
    subkeys = jax.random.split(jax.random.fold_in(key, 31), 3)
    slow_base = jax.random.uniform(subkeys[0], (HEAD_TOTAL,), jnp.float32, -7.0, -4.5)
    fast_base = jax.random.uniform(subkeys[1], (HEAD_TOTAL,), jnp.float32, -3.0, 0.0)
    base_level = jnp.where(chosen, slow_base, fast_base)
    data_part = 0.5 * jax.random.truncated_normal(subkeys[2], -4.0, 4.0, (TOKEN_TOTAL, HEAD_TOTAL), jnp.float32)
    return (base_level[None, :] + data_part).astype(jnp.bfloat16)


def draw_surge_decay(key, part):
    position_list = jax.random.permutation(jax.random.fold_in(key, 41), TOKEN_TOTAL)[:SURGE_POSITIONS].astype(jnp.int32)
    correction_scale = jax.random.uniform(jax.random.fold_in(key, 42), (SURGE_POSITIONS, HEAD_TOTAL), jnp.float32, 0.5, 0.8)
    hit_table = (jnp.arange(TOKEN_TOTAL, dtype=jnp.int32)[:, None] == position_list[None, :]).astype(jnp.float32)
    return jnp.dot(hit_table, jnp.log(correction_scale).astype(jnp.float32), precision=jax.lax.Precision.HIGHEST)


def level_of(key, dims, cuts, least, largest):
    factor_of, own = 1.0, jax.random.fold_in(key, 6)
    for axis_at, shards_of in cuts:
        steps = jnp.exp(jax.random.uniform(jax.random.fold_in(own, axis_at), (shards_of,), jnp.float32, least / len(cuts), largest / len(cuts)))
        factor_of = factor_of * jnp.repeat(steps, dims[axis_at] // shards_of).reshape([-1 if axis == axis_at else 1 for axis in range(len(dims))])
    return factor_of


def length_profile(count, total, bound, skew):
    weights = [(1 << 20) // math.isqrt(grade ** skew) + 1 for grade in range(2, count + 1)]
    spare, holding = total - bound - (count - 1), [1] * (count - 1)
    while spare > 0:
        free = [i for i in range(count - 1) if holding[i] < bound]
        whole, budget = sum([weights[i] for i in free]), spare
        for i in free:
            more = min(bound - holding[i], max(1, budget * weights[i] // whole), spare)
            holding[i] = holding[i] + more
            spare = spare - more
    return np.array([bound] + holding)


def ragged_sizes(key, amount, total, most, lean):
    if amount == 2:
        one = jax.random.randint(key, (), max(1, total - most), min(most, total - 1) + 1)
        return jnp.stack([one, total - one])
    lengths = jnp.asarray(length_profile(amount, total, most, lean), jnp.int32)
    pairs = (amount - 1) // 2
    donor, taker = lengths[1:1 + 2 * pairs:2], lengths[2:2 + 2 * pairs:2]
    room = jnp.minimum(donor - 1, most - taker)
    shifted = jax.random.randint(jax.random.fold_in(key, 1), (pairs,), 0, 1 << 20) % (room + 1)
    lengths = lengths.at[1:1 + 2 * pairs:2].set(donor - shifted).at[2:2 + 2 * pairs:2].set(taker + shifted)
    return lengths[jax.random.permutation(jax.random.fold_in(key, 2), amount)]


def assign_block(key, own, number, rows, number_of, top, reach, skew):
    order = jax.random.permutation(key, number_of)
    crowded, usual = shares(number_of, rows * top, reach, skew, True), shares(number_of, rows * top, reach, skew, False)
    places = jnp.arange(number_of)

    def named(lengths, turn):
        used = int((lengths > 0).sum())
        fixed = max(1, used // 4)
        moved = fixed + (places - fixed + turn * (used - fixed)) % max(1, number_of - fixed)
        return jnp.zeros((number_of,), jnp.int32).at[order[jnp.where(places < fixed, places, moved)]].set(jnp.asarray(lengths, jnp.int32))

    lengths = jnp.where(number % 4 == 0, named(crowded, number // 4), named(usual, number - number // 4 - 1))
    mixed = jax.random.permutation(jax.random.fold_in(own, 3), number_of)
    giver, receiver = mixed[0:number_of // 2 * 2:2], mixed[1:number_of // 2 * 2:2]
    room = jnp.minimum(lengths[giver] - 1, reach - lengths[receiver]) // 2
    room = jnp.where((giver == order[0]) | (receiver == order[0]) | (lengths[receiver] == 0), 0, jnp.maximum(room, 0))
    moved = jax.random.randint(jax.random.fold_in(own, 4), (number_of // 2,), 0, 1 << 20) % (room + 1)
    lengths = lengths.at[giver].add(-moved).at[receiver].add(moved)
    members = jnp.searchsorted(jnp.cumsum(lengths), jnp.arange(rows * top), side="right").astype(jnp.int32)
    grid = members.reshape(top, rows).T
    grid = grid[jax.random.permutation(jax.random.fold_in(own, 1), rows)]
    turn = jax.random.randint(jax.random.fold_in(own, 2), (rows, 1), 0, top)
    return jnp.take_along_axis(grid, (jnp.arange(top)[None, :] + turn) % top, axis=1)


def shares(number_of, total, reach, slope, full):
    loads = [(1 << 20) // math.isqrt(rank ** slope) + 1 for rank in range(1, number_of + 1)]
    largest = reach if full else min(reach, max(-(-total // number_of), total * loads[0] // sum(loads)))
    least = 1 if total - largest >= number_of - 1 else 0
    given, rest = [largest] + [least] * (number_of - 1), total - largest - least * (number_of - 1)
    while rest > 0:
        movable = [i for i in range(1, number_of) if given[i] < largest] or [i for i in range(1, number_of) if given[i] < reach]
        whole, budget = sum([loads[i] for i in movable]), rest
        for i in movable:
            addition = min(reach - given[i], max(1, budget * loads[i] // whole), rest)
            given[i] = given[i] + addition
            rest = rest - addition
    return np.array(given)


def normal_values(rng, dims, deviation, reach, cuts=(), held_as=jnp.bfloat16):
    level = level_of(rng, dims, cuts, -0.22, 0.18) if cuts else 1.0
    drawn = jax.random.normal(rng, dims, jnp.float32) * deviation * level
    return jnp.minimum(jnp.maximum(drawn, -reach), reach).astype(held_as)


def setup_inputs(seed: int = 0) -> dict:
    keys = jax.random.split(jax.random.key(seed), 20)
    head_queries = normal_values(keys[0], (TOKEN_TOTAL, D), 1.0, 6.0, ((0, 64), (1, 4)))
    head_keys = normal_values(keys[1], (TOKEN_TOTAL, D), 1.0, 6.0, ((0, 64), (1, 4)))
    head_values = normal_values(keys[2], (TOKEN_TOTAL, D), 1.0, 6.0, ((0, 64), (1, 4)))
    decay_logits = draw_decay_logits(jax.random.fold_in(keys[19], 71), 0)
    learning_logits = draw_learning_logits(jax.random.fold_in(keys[19], 71), 0)
    surge_decay = draw_surge_decay(jax.random.fold_in(keys[19], 71), 0)
    documents = jnp.searchsorted(jnp.cumsum(ragged_sizes(keys[6], DOCS, TOKEN_TOTAL, DOC_MOST, 1)), jnp.arange(TOKEN_TOTAL), side="right").astype(jnp.int32)
    residual = normal_values(keys[7], (TOKEN_TOTAL, D), 1.0, 6.0, ((0, 256),))
    head_norm_scale = jnp.clip(1.0 + 0.18 * jax.random.normal(keys[8], (D,), jnp.float32), 0.1, 1.9)
    mixer_output_weight = normal_values(keys[9], (D, D), D ** -0.5, 0.125, ((0, 4),))
    layer_norm_scale = jnp.clip(1.0 + 0.18 * jax.random.normal(keys[10], (D,), jnp.float32), 0.1, 1.9)
    routes_keys = jax.random.split(jax.random.fold_in(keys[11], 1), TOKEN_TOTAL // TOK_DEV)
    routes_turns = jax.random.permutation(jax.random.fold_in(keys[11], 3), TOKEN_TOTAL // TOK_DEV)
    routes = jax.vmap(lambda own, number: assign_block(jax.random.fold_in(keys[11], 2), own, number, TOK_DEV, EXPERTS, TOP, CAP, 2))(routes_keys, routes_turns).reshape((TOKEN_TOTAL, TOP))
    routing_weight = jnp.clip(jnp.exp(math.log(1.5) - 1.60943787 * jax.random.uniform(keys[12], (TOKEN_TOTAL, TOP), jnp.float32) ** level_of(keys[12], (TOKEN_TOTAL, TOP), ((0, 256),), -0.2, 0.2)), 0.3, 1.5)
    routed_gate_weight = normal_values(keys[13], (EXPERTS, D, FFE), D ** -0.5, 0.125, ((0, 64), (2, 4)))
    routed_up_weight = normal_values(keys[14], (EXPERTS, D, FFE), D ** -0.5, 0.125, ((0, 64), (2, 4)))
    routed_down_weight = normal_values(keys[15], (EXPERTS, FFE, D), FFE ** -0.5, 0.1875, ((0, 64), (1, 4)))
    common_gate_weight = normal_values(keys[16], (D, SFF), D ** -0.5, 0.125, ((1, 4),))
    common_up_weight = normal_values(keys[17], (D, SFF), D ** -0.5, 0.125, ((1, 4),))
    common_down_weight = normal_values(keys[18], (SFF, D), SFF ** -0.5, 0.25, ((0, 4),))
    return dict(head_queries=head_queries, head_keys=head_keys, head_values=head_values, decay_logits=decay_logits, learning_logits=learning_logits, surge_decay=surge_decay, documents=documents, residual=residual, head_norm_scale=head_norm_scale, mixer_output_weight=mixer_output_weight, layer_norm_scale=layer_norm_scale, routes=routes, routing_weight=routing_weight, routed_gate_weight=routed_gate_weight, routed_up_weight=routed_up_weight, routed_down_weight=routed_down_weight, common_gate_weight=common_gate_weight, common_up_weight=common_up_weight, common_down_weight=common_down_weight)


residual_scale = 2.0 ** 0.5
group_eps = 0.00064
norm_eps = 1e-05
unit_eps = 1e-06
highest = lax.Precision.HIGHEST

def linear_recurrence_mixer(head_queries, head_keys, head_values, decay_logits, learning_logits, surge_decay, documents, head_norm_scale):
    shape_three = (TOKEN_TOTAL, HEAD_TOTAL, HEAD)
    read_heads = head_queries.astype(jnp.float32).reshape(shape_three)
    key_heads = head_keys.astype(jnp.float32).reshape(shape_three)
    value_heads = head_values.astype(jnp.float32).reshape(shape_three)
    unit_keys = key_heads * lax.rsqrt(lax.optimization_barrier(jnp.sum(key_heads * key_heads, -1, keepdims=True)) + unit_eps)
    learn_rate = jax.nn.sigmoid(learning_logits.astype(jnp.float32))
    decay_logarithm = (-jnp.exp(-jax.nn.softplus(-decay_logits.astype(jnp.float32)) - 0.5)).reshape(shape_three)
    decay_logarithm = decay_logarithm + surge_decay[:, :, None]
    keeping = jnp.concatenate([jnp.zeros((1,), jnp.float32), (documents[1:] == documents[:-1]).astype(jnp.float32)])

    def advance(carried, inputs):
        read_now, key_now, value_now, unit_now, rate_now, decay_now, keep_now = inputs
        pulled = jnp.einsum('hvk,hk->hv', carried, unit_now, precision=highest)
        carried = keep_now * (carried * jnp.exp(decay_now)[:, None, :] - (rate_now[:, None] * pulled)[:, :, None] * unit_now[:, None, :])
        carried = carried + value_now[:, :, None] * key_now[:, None, :]
        return (carried, jnp.einsum('hvk,hk->hv', carried, read_now, precision=highest))
    initial = jnp.zeros((HEAD_TOTAL, HEAD, HEAD), jnp.float32)
    _, head_read = lax.scan(advance, initial, (read_heads, key_heads, value_heads, unit_keys, learn_rate, decay_logarithm, keeping))
    centre = lax.optimization_barrier(jnp.mean(head_read, -1, keepdims=True))
    spread = lax.optimization_barrier(jnp.mean(jnp.square(head_read - centre), -1, keepdims=True))
    normed = ((head_read - centre) * lax.rsqrt(spread + group_eps)).reshape(TOKEN_TOTAL, D) * head_norm_scale
    return normed.astype(jnp.bfloat16)

def rounded(values):
    return lax.optimization_barrier(values.astype(jnp.bfloat16)).astype(jnp.float32)

def split_down(hidden, down):
    block_width = hidden.shape[1] // N_TP
    pieces = jnp.einsum('rjf,jfd->jrd', hidden.reshape(hidden.shape[0], N_TP, block_width).astype(jnp.float32), down.reshape(N_TP, block_width, D).astype(jnp.float32))
    return lax.optimization_barrier(jnp.sum(rounded(pieces), 0))

def swiglu_hidden(rows_in, gate, upward):
    gated = jnp.dot(rows_in, gate, preferred_element_type=jnp.float32)
    lifted = jnp.dot(rows_in, upward, preferred_element_type=jnp.float32)
    return (jax.nn.silu(gated) * lifted).astype(jnp.bfloat16)

def reference(head_queries, head_keys, head_values, decay_logits, learning_logits, surge_decay, documents, residual, head_norm_scale, mixer_output_weight, layer_norm_scale, routes, routing_weight, routed_gate_weight, routed_up_weight, routed_down_weight, common_gate_weight, common_up_weight, common_down_weight):
    head_outputs = linear_recurrence_mixer(head_queries, head_keys, head_values, decay_logits, learning_logits, surge_decay, documents, head_norm_scale)
    block_width = D // N_TP
    mixed_rows = jnp.zeros((TOKEN_TOTAL, D), jnp.float32)
    for block_index in range(N_TP):
        lower = block_index * block_width
        mixed_rows = mixed_rows + rounded(jnp.dot(head_outputs[:, lower:lower + block_width], mixer_output_weight[lower:lower + block_width], preferred_element_type=jnp.float32))
    summed = residual_scale * residual.astype(jnp.float32) + mixed_rows
    centre = lax.optimization_barrier(jnp.mean(summed, -1, keepdims=True))
    spread = lax.optimization_barrier(jnp.mean(jnp.square(summed - centre), -1, keepdims=True))
    stream = ((summed - centre) * lax.rsqrt(spread + norm_eps) * layer_norm_scale).astype(jnp.bfloat16)
    devices = N_SP * N_TP
    chosen = routes.reshape(devices, TOK_DEV * TOP)
    onehot = (chosen[..., None] == jnp.arange(EXPERTS, dtype=jnp.int32)).astype(jnp.int32)
    ranking = (lax.optimization_barrier(jnp.sum(jnp.cumsum(onehot, 1) * onehot, -1)) - 1).astype(jnp.int32)
    device_ids = jnp.arange(devices, dtype=jnp.int32)[:, None]
    slot_index = (chosen * (devices * CAP) + device_ids * CAP + ranking).reshape(-1).astype(jnp.int32)
    buffer = jnp.zeros((EXPERTS * devices * CAP, D), jnp.bfloat16).at[slot_index].set(jnp.repeat(stream, TOP, axis=0))

    def one_expert(operands):
        rows_in, gate, upward, down = operands
        return split_down(swiglu_hidden(rows_in, gate, upward), down).astype(jnp.bfloat16)
    results = lax.map(one_expert, (buffer.reshape(EXPERTS, devices * CAP, D), routed_gate_weight, routed_up_weight, routed_down_weight))
    picked = results.reshape(EXPERTS * devices * CAP, D)[slot_index].astype(jnp.float32).reshape(TOKEN_TOTAL, TOP, D)
    routed = lax.optimization_barrier(jnp.sum(picked * routing_weight[:, :, None], 1))

    def shared_block(rows_in):
        return split_down(swiglu_hidden(rows_in, common_gate_weight, common_up_weight), common_down_weight)
    shared_rows = lax.map(shared_block, stream.reshape(N_SP, TOKEN_TOTAL // N_SP, D)).reshape(TOKEN_TOTAL, D)
    return (residual_scale * stream.astype(jnp.float32) + routed + shared_rows).astype(jnp.bfloat16)
```

```python
import functools
import jax
import jax.numpy as jnp
from jax import lax
from jax.experimental import pallas as pl
from jax.experimental.pallas import tpu as pltpu
from jax.sharding import PartitionSpec as P

HEAD = 64
PAIR = 128
SPAN = 64
REACH = 6
EXP_DEV = 2
TOP = 2
TOK_DEV = 64

residual_scale = 2.0**0.5
group_eps = 0.00064
norm_eps = 1e-05
unit_eps = 1e-06
F32, BF16 = jnp.float32, jnp.bfloat16

NN = (((1,), (0,)), ((), ()))
NT = (((1,), (1,)), ((), ()))
TN = (((0,), (0,)), ((), ()))


def iota(rows, cols, axis):
    return lax.broadcasted_iota(jnp.int32, (rows, cols), axis)


def mm(a, b, dims=NN):
    return lax.dot_general(a, b, dims, preferred_element_type=F32)


def halves(x):
    high = x.astype(BF16)
    return high, (x - high.astype(F32)).astype(BF16)


def thirds(x):
    high = x.astype(BF16)
    rest = x - high.astype(F32)
    mid = rest.astype(BF16)
    return high, mid, (rest - mid.astype(F32)).astype(BF16)


def mm3(a, b, dims=NN):
    return mm(a[0], b[0], dims) + (mm(a[1], b[0], dims) + mm(a[0], b[1], dims))


def exact_right(a, b):
    one, two, three = thirds(b)
    return mm(a, one) + (mm(a, two) + mm(a, three))


def head_masks():
    lane = iota(1, PAIR, 1)
    return (lane < HEAD).astype(F32).astype(BF16), (lane >= HEAD).astype(F32).astype(BF16)


def spread_one(x, masks):
    return jnp.concatenate([x * masks[0], x * masks[1]], axis=0)


def spread(pair, masks):
    return tuple(spread_one(x, masks) for x in pair)


def beside(a, b, axis):
    return tuple(jnp.concatenate([x, y], axis=axis) for x, y in zip(a, b))


def local_kernel(
    q_ref, k_ref, v_ref, dec_ref, rate_ref, surge_ref, doc_ref,
    pay_ref, ru_ref, rkv_ref, cm_ref, lp_ref, fj_ref, state_ref,
):
    pair = pl.program_id(0)
    length = q_ref.shape[0]
    blocks = length // SPAN
    masks = head_masks()
    head_same = iota(PAIR, PAIR, 0) // HEAD == iota(PAIR, PAIR, 1) // HEAD
    queries, keys, values = (r[...].astype(F32) for r in (q_ref, k_ref, v_ref))
    chosen = (iota(8, PAIR, 0) == 2 * pair + iota(8, PAIR, 1) // HEAD).astype(F32)
    rates = 1.0 / (1.0 + jnp.exp(-rate_ref[...].astype(F32)))
    rate = jnp.dot(rates, chosen, precision=lax.Precision.HIGHEST, preferred_element_type=F32)
    surge = jnp.dot(
        surge_ref[...], chosen, precision=lax.Precision.HIGHEST, preferred_element_type=F32
    )
    same = head_same.astype(F32).astype(BF16)
    one, two = halves(keys * keys)
    unit = keys * lax.rsqrt(mm(one, same) + mm(two, same) + unit_eps)
    decay = surge - 0.6065306597126334 / (1.0 + jnp.exp(-dec_ref[...].astype(F32)))
    row, col = iota(length, length, 0), iota(length, length, 1)
    lower = ((row // SPAN == col // SPAN) & (col <= row)).astype(F32).astype(BF16)
    cumulative = exact_right(lower, decay)
    back, ahead = jnp.exp(-cumulative), jnp.exp(cumulative - decay)
    ahead_unit = unit * ahead
    back_unit = unit * rate * back
    back_key = keys * back
    forward = queries * jnp.exp(cumulative)
    docs_row = doc_ref[...].astype(F32)
    diagonal = jnp.where(row == col, jnp.broadcast_to(docs_row, (length, length)), 0.0)
    docs = mm(diagonal.astype(BF16), jnp.ones((length, PAIR), BF16))
    pick = (iota(SPAN, PAIR, 1) == 0).astype(F32).astype(BF16)
    t_pos, s_pos = iota(SPAN, PAIR, 0), iota(SPAN, PAIR, 1) % HEAD
    eye = (t_pos == s_pos).astype(F32)
    big_eye = iota(PAIR, PAIR, 0) == iota(PAIR, PAIR, 1)
    carried = through = None
    for b in range(blocks):
        at = slice(b * SPAN, (b + 1) * SPAN)
        doc = docs[at]
        prior = docs[max(b * SPAN - 1, 0) : max(b * SPAN - 1, 0) + 1]
        joined = (doc == prior).astype(F32)
        tail = (doc == doc[SPAN - 1 :]).astype(F32)
        doc16 = doc.astype(BF16)
        doc_s = mm(pick, jnp.concatenate([doc16, doc16], 0), NT)
        same_doc = doc == doc_s
        strict = same_doc & (t_pos > s_pos)
        causal = same_doc & (t_pos >= s_pos)
        left = halves(jnp.concatenate([ahead_unit[at], forward[at]], 0))
        right = beside(
            spread(halves(back_unit[at]), masks), spread(halves(back_key[at]), masks), 0
        )
        scores = mm3(left, right, NT)
        inner = jnp.where(strict, scores[:SPAN, :PAIR], 0.0)
        mix_key = jnp.where(strict, scores[:SPAN, PAIR:], 0.0)
        read_unit = jnp.where(causal, -scores[SPAN:, :PAIR], 0.0)
        read_key = jnp.where(causal, scores[SPAN:, PAIR:], 0.0)
        near = jnp.where(t_pos // 16 == s_pos // 16, inner, 0.0)
        x = eye - near
        n_pair = halves(near)
        power = mm3(n_pair, spread(n_pair, masks))
        for step in range(3):
            p_pair = halves(power)
            p_wide = spread(p_pair, masks)
            if step < 2:
                both = mm3(beside(halves(x), p_pair, 0), p_wide)
                x, power = x + both[:SPAN], both[SPAN:]
            else:
                x = x + mm3(halves(x), p_wide)
        for width in (32, 64):
            cross = (t_pos // width == s_pos // width) & (
                t_pos // (width // 2) != s_pos // (width // 2)
            )
            part = spread(halves(jnp.where(cross, inner, 0.0)), masks)
            x_pair = halves(x)
            x = x - mm3(halves(mm3(x_pair, part)), spread(x_pair, masks))
        value = values[at].astype(BF16)
        value_wide = spread_one(value, masks)
        weights = halves(jnp.concatenate([mix_key, read_key], 0))
        weighed = mm(weights[0], value_wide) + mm(weights[1], value_wide)
        rkv_ref[0, at] = weighed[SPAN:]
        side = beside(
            spread(halves(ahead_unit[at] * joined), masks),
            spread(halves(weighed[:SPAN]), masks),
            1,
        )
        solved = mm3(halves(x), side)
        carry_map, local_pull = solved[:, :PAIR], solved[:, PAIR:]
        ru_ref[0, at] = read_unit
        cm_ref[0, at] = carry_map
        lp_ref[0, at] = local_pull
        fj_ref[0, at] = forward[at] * joined
        total = cumulative[b * SPAN + SPAN - 1 : b * SPAN + SPAN]
        to_end = jnp.exp(total - cumulative[at]) * tail
        end_unit = halves(unit[at] * (to_end * -rate[at]))
        end_key = halves(keys[at] * to_end)
        block_map = mm3(halves(carry_map), end_unit, TN)
        block_map = jnp.where(head_same, block_map, 0.0) + jnp.where(
            big_eye, jnp.exp(total) * joined[SPAN - 1 :], 0.0
        )
        add = mm3(halves(local_pull), end_unit, TN) + (
            mm(value, end_key[0], TN) + mm(value, end_key[1], TN)
        )
        add = jnp.where(head_same, add, 0.0)
        add = add[:HEAD] + add[HEAD:]
        if b == 0:
            state_ref[0, 0] = jnp.concatenate([jnp.zeros((HEAD, PAIR), F32), eye], 0)
            carried, through = add, block_map[:HEAD] + block_map[HEAD:]
        else:
            before = jnp.concatenate([carried, through], 0)
            state_ref[0, b] = before
            after = mm3(halves(before), halves(block_map))
            carried, through = after[:HEAD] + add, after[HEAD:]
    pay_ref[0, :HEAD] = through.astype(BF16)
    pay_ref[0, HEAD : 2 * HEAD] = carried.astype(BF16)
    pay_ref[0, 2 * HEAD :] = jnp.broadcast_to(docs[length - 1 :], (16, PAIR)).astype(BF16)


def outputs_kernel(ru_ref, rkv_ref, cm_ref, lp_ref, fj_ref, state_ref, out_ref, start_ref):
    masks = head_masks()
    for b in range(ru_ref.shape[1] // SPAN):
        at = slice(b * SPAN, (b + 1) * SPAN)
        side = beside(
            spread(halves(cm_ref[0, at]), masks), spread(halves(lp_ref[0, at]), masks), 1
        )
        z = mm3(halves(ru_ref[0, at]), side)
        begin = halves(fj_ref[0, at] + z[:, :PAIR])
        states = halves(state_ref[0, b])
        wide = beside(
            spread(tuple(s[:HEAD] for s in states), masks),
            spread(tuple(s[HEAD:] for s in states), masks),
            0,
        )
        y = mm3(begin, wide, NT)
        out_ref[0, at] = rkv_ref[0, at] + z[:, PAIR:] + y[:, :PAIR]
        start_ref[0, at] = y[:, PAIR:]


def finish_kernel(out_ref, start_ref, doc_ref, scale_ref, w_ref, *rest):
    pays, mixed_ref, heads = rest[:REACH], rest[REACH], rest[REACH + 1]
    masks = head_masks()
    same = (iota(PAIR, PAIR, 0) // HEAD == iota(PAIR, PAIR, 1) // HEAD).astype(F32)
    same = (same * (1.0 / HEAD)).astype(BF16)
    first = jnp.broadcast_to(doc_ref[:, :1].astype(F32), (1, PAIR))

    def mean(x):
        one, two = halves(x)
        return mm(one, same) + mm(two, same)

    for pair in range(out_ref.shape[0]):
        state = None
        for j in range(REACH - 1, -1, -1):
            pay = pays[j]
            linked = pay[pair, 2 * HEAD : 2 * HEAD + 1].astype(F32) == first
            add = pay[pair, HEAD : 2 * HEAD].astype(F32)
            if state is not None:
                wide = spread_one(pay[pair, :HEAD], masks)
                one, two = halves(state)
                add = add + (mm(one, wide) + mm(two, wide))
            state = jnp.where(linked, add, 0.0)
        wide = spread(halves(state), masks)
        read = out_ref[pair] + mm3(halves(start_ref[pair]), wide, NT)
        centred = read - mean(read)
        normed = centred * lax.rsqrt(mean(centred * centred) + group_eps)
        lanes = slice(pair * PAIR, (pair + 1) * PAIR)
        heads[:, lanes] = (normed * scale_ref[:, lanes]).astype(BF16)
    mixed_ref[...] = mm(heads[...], w_ref[...]).astype(BF16)


def sds(shape, dtype):
    return jax.ShapeDtypeStruct(shape, dtype)


def mixer(q, k, v, dec, rate, surge, documents, scale, weight, interpret=False):
    length, width = q.shape
    pairs = width // PAIR
    blocks = length // SPAN
    docs = documents.reshape(1, length)
    wide = pl.BlockSpec((length, PAIR), lambda p: (0, p))
    whole = lambda a: pl.BlockSpec(a.shape, lambda p: (0,) * a.ndim)
    part = lambda *dims: pl.BlockSpec((1, *dims), lambda p: (p,) + (0,) * len(dims))
    mid_shapes = [(length, PAIR)] * 5 + [(blocks, PAIR, PAIR)]
    local = pl.pallas_call(
        local_kernel,
        grid=(pairs,),
        in_specs=[wide] * 4 + [whole(rate), whole(surge), whole(docs)],
        out_specs=[part(2 * HEAD + 16, PAIR)] + [part(*s) for s in mid_shapes],
        out_shape=[sds((pairs, 2 * HEAD + 16, PAIR), BF16)]
        + [sds((pairs, *s), F32) for s in mid_shapes],
        cost_estimate=pl.CostEstimate(
            flops=6_000_000_000, bytes_accessed=6_000_000, transcendentals=600_000
        ),
        name="mixer_local",
        interpret=interpret,
    )
    pay, *mids = local(q, k, v, dec, rate, surge, docs)
    devices = lax.axis_size("sp")
    pays = [
        lax.ppermute(pay, "sp", [(d, (d + j) % devices) for d in range(devices)])
        for j in range(1, REACH + 1)
    ]
    outs = pl.pallas_call(
        outputs_kernel,
        grid=(pairs,),
        in_specs=[part(*s) for s in mid_shapes],
        out_specs=[part(length, PAIR)] * 2,
        out_shape=[sds((pairs, length, PAIR), F32)] * 2,
        cost_estimate=pl.CostEstimate(
            flops=5_000_000_000, bytes_accessed=6_000_000, transcendentals=0
        ),
        name="mixer_outputs",
        interpret=interpret,
    )(*mids)
    return pl.pallas_call(
        finish_kernel,
        out_shape=sds((length, weight.shape[1]), BF16),
        scratch_shapes=[pltpu.VMEM((length, width), BF16)],
        cost_estimate=pl.CostEstimate(
            flops=1_000_000_000, bytes_accessed=6_000_000, transcendentals=200_000
        ),
        name="mixer_finish",
        interpret=interpret,
    )(*outs, docs, scale.reshape(1, width), weight, *pays)


def split_up(x, dim, devices):
    shape = x.shape
    pieces = x.reshape(*shape[:dim], devices, shape[dim] // devices, *shape[dim + 1 :])
    return jnp.moveaxis(pieces, dim, 0)


def sent_and_summed(x, axis, dim):
    pieces = split_up(x, dim, lax.axis_size(axis))
    arrived = lax.all_to_all(pieces, axis, split_axis=0, concat_axis=0, tiled=True)
    return arrived.astype(jnp.float32).sum(axis=0)


def per_device(
    head_queries,
    head_keys,
    head_values,
    decay_logits,
    learning_logits,
    surge_decay,
    documents,
    residual,
    head_norm_scale,
    mixer_output_weight,
    layer_norm_scale,
    routes,
    routing_weight,
    routed_gate_weight,
    routed_up_weight,
    routed_down_weight,
    common_gate_weight,
    common_up_weight,
    common_down_weight,
):
    mixed = mixer(
        head_queries,
        head_keys,
        head_values,
        decay_logits,
        learning_logits,
        surge_decay,
        documents,
        head_norm_scale,
        mixer_output_weight,
    )
    mixed_rows = sent_and_summed(mixed, "tp", 0)
    summed = residual_scale * residual.astype(jnp.float32) + mixed_rows
    centre = jnp.mean(summed, -1, keepdims=True)
    spread = jnp.mean(jnp.square(summed - centre), -1, keepdims=True)
    stream = ((summed - centre) * lax.rsqrt(spread + norm_eps) * layer_norm_scale).astype(
        jnp.bfloat16
    )
    quarters = lax.axis_size("tp")
    groups = lax.axis_size("sp")
    experts = EXP_DEV * groups
    capacity = 2
    own_rows, model_width = stream.shape
    chosen = routes.reshape(quarters, own_rows * TOP)
    onehot = (chosen[..., None] == jnp.arange(experts, dtype=jnp.int32)).astype(jnp.int32)
    ranking = jnp.sum(jnp.cumsum(onehot, 1) * onehot, -1) - 1
    slot_index = chosen * capacity + ranking
    own_slots = lax.dynamic_index_in_dim(slot_index, lax.axis_index("tp"), 0, keepdims=False)
    outgoing = jnp.zeros((experts * capacity, model_width), jnp.bfloat16)
    outgoing = outgoing.at[own_slots].set(jnp.repeat(stream, TOP, axis=0))
    arrived = lax.all_to_all(
        outgoing.reshape(groups, EXP_DEV, capacity, model_width),
        "sp",
        split_axis=0,
        concat_axis=0,
        tiled=True,
    )
    arrived_all, rows_all = (
        lax.all_gather(arrived[None], "tp", axis=0, tiled=True),
        lax.all_gather(stream, "tp", axis=0, tiled=True),
    )
    gated = jnp.einsum(
        "qsecd,edf->qsecf", arrived_all, routed_gate_weight, preferred_element_type=jnp.float32
    )
    lifted = jnp.einsum(
        "qsecd,edf->qsecf", arrived_all, routed_up_weight, preferred_element_type=jnp.float32
    )
    hidden = (jax.nn.silu(gated) * lifted).astype(jnp.bfloat16)
    partial_value = jnp.einsum(
        "qsecf,efd->qsecd", hidden, routed_down_weight, preferred_element_type=jnp.float32
    )
    shared_gated = jnp.dot(rows_all, common_gate_weight, preferred_element_type=jnp.float32)
    shared_lifted = jnp.dot(rows_all, common_up_weight, preferred_element_type=jnp.float32)
    shared_hidden = (jax.nn.silu(shared_gated) * shared_lifted).astype(jnp.bfloat16)
    shared_part = jnp.dot(shared_hidden, common_down_weight, preferred_element_type=jnp.float32)
    expert_sum, shared_sum = (
        sent_and_summed(partial_value.astype(jnp.bfloat16), "tp", 0),
        sent_and_summed(shared_part.astype(jnp.bfloat16), "tp", 0),
    )
    returned = lax.all_to_all(
        expert_sum[0].astype(jnp.bfloat16), "sp", split_axis=0, concat_axis=0, tiled=True
    )
    picked = returned.reshape(experts * capacity, model_width)[own_slots]
    weighted = (
        picked.astype(jnp.float32).reshape(own_rows, TOP, model_width) * routing_weight[:, :, None]
    )
    routed = jnp.sum(weighted, 1)
    return (residual_scale * stream.astype(jnp.float32) + routed + shared_sum).astype(jnp.bfloat16)


def solution(mesh):
    rows = P("sp", "tp")
    own = P(("sp", "tp"), None)
    placed = (
        *(rows,) * 6,
        P("sp"),
        own,
        P("tp"),
        P("tp", None),
        P(),
        P("sp", None),
        own,
        P("sp", None, "tp"),
        P("sp", None, "tp"),
        P("sp", "tp", None),
        P(None, "tp"),
        P(None, "tp"),
        P("tp", None),
    )
    return jax.shard_map(
        per_device, mesh=mesh, in_specs=placed, out_specs=own, check_vma=False
    )
```

```python
import functools
import jax
import jax.numpy as jnp
from jax import lax
from jax.experimental import pallas as pl
from jax.experimental.pallas import tpu as pltpu
from jax.sharding import Mesh
from jax.sharding import PartitionSpec as P

HEAD = 64
PAIR = 128
SPAN = 64
REACH = 6
EXP_DEV = 2
TOP = 2
TOK_DEV = 64

residual_scale = 2.0**0.5
group_eps = 0.00064
norm_eps = 1e-05
unit_eps = 1e-06
F32, BF16 = jnp.float32, jnp.bfloat16

NN = (((1,), (0,)), ((), ()))
NT = (((1,), (1,)), ((), ()))
TN = (((0,), (0,)), ((), ()))


def iota(rows, cols, axis):
    return lax.broadcasted_iota(jnp.int32, (rows, cols), axis)


def mm(a, b, dims=NN):
    return lax.dot_general(a, b, dims, preferred_element_type=F32)


def halves(x):
    high = x.astype(BF16)
    return high, (x - high.astype(F32)).astype(BF16)


def thirds(x):
    high = x.astype(BF16)
    rest = x - high.astype(F32)
    mid = rest.astype(BF16)
    return high, mid, (rest - mid.astype(F32)).astype(BF16)


def mm3(a, b, dims=NN):
    return mm(a[0], b[0], dims) + (mm(a[1], b[0], dims) + mm(a[0], b[1], dims))


def exact_right(a, b):
    one, two, three = thirds(b)
    return mm(a, one) + (mm(a, two) + mm(a, three))


def head_masks():
    lane = iota(1, PAIR, 1)
    return (lane < HEAD).astype(F32).astype(BF16), (lane >= HEAD).astype(F32).astype(BF16)


def spread_one(x, masks):
    return jnp.concatenate([x * masks[0], x * masks[1]], axis=0)


def spread(pair, masks):
    return tuple(spread_one(x, masks) for x in pair)


def beside(a, b, axis):
    return tuple(jnp.concatenate([x, y], axis=axis) for x, y in zip(a, b))


def local_kernel(
    q_ref, k_ref, v_ref, dec_ref, rate_ref, surge_ref, doc_ref,
    pay_ref, ru_ref, rkv_ref, cm_ref, lp_ref, fj_ref, state_ref,
):
    pair = pl.program_id(0)
    length = q_ref.shape[0]
    blocks = length // SPAN
    masks = head_masks()
    head_same = iota(PAIR, PAIR, 0) // HEAD == iota(PAIR, PAIR, 1) // HEAD
    queries, keys, values = (r[...].astype(F32) for r in (q_ref, k_ref, v_ref))
    chosen = (iota(8, PAIR, 0) == 2 * pair + iota(8, PAIR, 1) // HEAD).astype(F32)
    rates = 1.0 / (1.0 + jnp.exp(-rate_ref[...].astype(F32)))
    rate = jnp.dot(rates, chosen, precision=lax.Precision.HIGHEST, preferred_element_type=F32)
    surge = jnp.dot(
        surge_ref[...], chosen, precision=lax.Precision.HIGHEST, preferred_element_type=F32
    )
    same = head_same.astype(F32).astype(BF16)
    one, two = halves(keys * keys)
    unit = keys * lax.rsqrt(mm(one, same) + mm(two, same) + unit_eps)
    decay = surge - 0.6065306597126334 / (1.0 + jnp.exp(-dec_ref[...].astype(F32)))
    row, col = iota(length, length, 0), iota(length, length, 1)
    lower = ((row // SPAN == col // SPAN) & (col <= row)).astype(F32).astype(BF16)
    cumulative = exact_right(lower, decay)
    back, ahead = jnp.exp(-cumulative), jnp.exp(cumulative - decay)
    ahead_unit = unit * ahead
    back_unit = unit * rate * back
    back_key = keys * back
    forward = queries * jnp.exp(cumulative)
    docs_row = doc_ref[...].astype(F32)
    diagonal = jnp.where(row == col, jnp.broadcast_to(docs_row, (length, length)), 0.0)
    docs = mm(diagonal.astype(BF16), jnp.ones((length, PAIR), BF16))
    pick = (iota(SPAN, PAIR, 1) == 0).astype(F32).astype(BF16)
    t_pos, s_pos = iota(SPAN, PAIR, 0), iota(SPAN, PAIR, 1) % HEAD
    eye = (t_pos == s_pos).astype(F32)
    big_eye = iota(PAIR, PAIR, 0) == iota(PAIR, PAIR, 1)
    carried = through = None
    for b in range(blocks):
        at = slice(b * SPAN, (b + 1) * SPAN)
        doc = docs[at]
        prior = docs[max(b * SPAN - 1, 0) : max(b * SPAN - 1, 0) + 1]
        joined = (doc == prior).astype(F32)
        tail = (doc == doc[SPAN - 1 :]).astype(F32)
        doc16 = doc.astype(BF16)
        doc_s = mm(pick, jnp.concatenate([doc16, doc16], 0), NT)
        same_doc = doc == doc_s
        strict = same_doc & (t_pos > s_pos)
        causal = same_doc & (t_pos >= s_pos)
        left = halves(jnp.concatenate([ahead_unit[at], forward[at]], 0))
        right = beside(
            spread(halves(back_unit[at]), masks), spread(halves(back_key[at]), masks), 0
        )
        scores = mm3(left, right, NT)
        inner = jnp.where(strict, scores[:SPAN, :PAIR], 0.0)
        mix_key = jnp.where(strict, scores[:SPAN, PAIR:], 0.0)
        read_unit = jnp.where(causal, -scores[SPAN:, :PAIR], 0.0)
        read_key = jnp.where(causal, scores[SPAN:, PAIR:], 0.0)
        near = jnp.where(t_pos // 16 == s_pos // 16, inner, 0.0)
        x = eye - near
        n_pair = halves(near)
        power = mm3(n_pair, spread(n_pair, masks))
        for step in range(3):
            p_pair = halves(power)
            p_wide = spread(p_pair, masks)
            if step < 2:
                both = mm3(beside(halves(x), p_pair, 0), p_wide)
                x, power = x + both[:SPAN], both[SPAN:]
            else:
                x = x + mm3(halves(x), p_wide)
        for width in (32, 64):
            cross = (t_pos // width == s_pos // width) & (
                t_pos // (width // 2) != s_pos // (width // 2)
            )
            part = spread(halves(jnp.where(cross, inner, 0.0)), masks)
            x_pair = halves(x)
            x = x - mm3(halves(mm3(x_pair, part)), spread(x_pair, masks))
        value = values[at].astype(BF16)
        value_wide = spread_one(value, masks)
        weights = halves(jnp.concatenate([mix_key, read_key], 0))
        weighed = mm(weights[0], value_wide) + mm(weights[1], value_wide)
        rkv_ref[0, at] = weighed[SPAN:]
        side = beside(
            spread(halves(ahead_unit[at] * joined), masks),
            spread(halves(weighed[:SPAN]), masks),
            1,
        )
        solved = mm3(halves(x), side)
        carry_map, local_pull = solved[:, :PAIR], solved[:, PAIR:]
        ru_ref[0, at] = read_unit
        cm_ref[0, at] = carry_map
        lp_ref[0, at] = local_pull
        fj_ref[0, at] = forward[at] * joined
        total = cumulative[b * SPAN + SPAN - 1 : b * SPAN + SPAN]
        to_end = jnp.exp(total - cumulative[at]) * tail
        end_unit = halves(unit[at] * (to_end * -rate[at]))
        end_key = halves(keys[at] * to_end)
        block_map = mm3(halves(carry_map), end_unit, TN)
        block_map = jnp.where(head_same, block_map, 0.0) + jnp.where(
            big_eye, jnp.exp(total) * joined[SPAN - 1 :], 0.0
        )
        add = mm3(halves(local_pull), end_unit, TN) + (
            mm(value, end_key[0], TN) + mm(value, end_key[1], TN)
        )
        add = jnp.where(head_same, add, 0.0)
        add = add[:HEAD] + add[HEAD:]
        if b == 0:
            state_ref[0, 0] = jnp.concatenate([jnp.zeros((HEAD, PAIR), F32), eye], 0)
            carried, through = add, block_map[:HEAD] + block_map[HEAD:]
        else:
            before = jnp.concatenate([carried, through], 0)
            state_ref[0, b] = before
            after = mm3(halves(before), halves(block_map))
            carried, through = after[:HEAD] + add, after[HEAD:]
    pay_ref[0, :HEAD] = through.astype(BF16)
    pay_ref[0, HEAD : 2 * HEAD] = carried.astype(BF16)
    pay_ref[0, 2 * HEAD :] = jnp.broadcast_to(docs[length - 1 :], (16, PAIR)).astype(BF16)


def outputs_kernel(ru_ref, rkv_ref, cm_ref, lp_ref, fj_ref, state_ref, out_ref, start_ref):
    masks = head_masks()
    for b in range(ru_ref.shape[1] // SPAN):
        at = slice(b * SPAN, (b + 1) * SPAN)
        side = beside(
            spread(halves(cm_ref[0, at]), masks), spread(halves(lp_ref[0, at]), masks), 1
        )
        z = mm3(halves(ru_ref[0, at]), side)
        begin = halves(fj_ref[0, at] + z[:, :PAIR])
        states = halves(state_ref[0, b])
        wide = beside(
            spread(tuple(s[:HEAD] for s in states), masks),
            spread(tuple(s[HEAD:] for s in states), masks),
            0,
        )
        y = mm3(begin, wide, NT)
        out_ref[0, at] = rkv_ref[0, at] + z[:, PAIR:] + y[:, :PAIR]
        start_ref[0, at] = y[:, PAIR:]


def finish_kernel(out_ref, start_ref, doc_ref, scale_ref, w_ref, *rest):
    pays, mixed_ref, heads = rest[:REACH], rest[REACH], rest[REACH + 1]
    masks = head_masks()
    same = (iota(PAIR, PAIR, 0) // HEAD == iota(PAIR, PAIR, 1) // HEAD).astype(F32)
    same = (same * (1.0 / HEAD)).astype(BF16)
    first = jnp.broadcast_to(doc_ref[:, :1].astype(F32), (1, PAIR))

    def mean(x):
        one, two = halves(x)
        return mm(one, same) + mm(two, same)

    for pair in range(out_ref.shape[0]):
        state = None
        for j in range(REACH - 1, -1, -1):
            pay = pays[j]
            linked = pay[pair, 2 * HEAD : 2 * HEAD + 1].astype(F32) == first
            add = pay[pair, HEAD : 2 * HEAD].astype(F32)
            if state is not None:
                wide = spread_one(pay[pair, :HEAD], masks)
                one, two = halves(state)
                add = add + (mm(one, wide) + mm(two, wide))
            state = jnp.where(linked, add, 0.0)
        wide = spread(halves(state), masks)
        read = out_ref[pair] + mm3(halves(start_ref[pair]), wide, NT)
        centred = read - mean(read)
        normed = centred * lax.rsqrt(mean(centred * centred) + group_eps)
        lanes = slice(pair * PAIR, (pair + 1) * PAIR)
        heads[:, lanes] = (normed * scale_ref[:, lanes]).astype(BF16)
    mixed_ref[...] = mm(heads[...], w_ref[...]).astype(BF16)


def sds(shape, dtype):
    return jax.ShapeDtypeStruct(shape, dtype)


def mixer(q, k, v, dec, rate, surge, documents, scale, weight, interpret=False):
    length, width = q.shape
    pairs = width // PAIR
    blocks = length // SPAN
    docs = documents.reshape(1, length)
    wide = pl.BlockSpec((length, PAIR), lambda p: (0, p))
    whole = lambda a: pl.BlockSpec(a.shape, lambda p: (0,) * a.ndim)
    part = lambda *dims: pl.BlockSpec((1, *dims), lambda p: (p,) + (0,) * len(dims))
    mid_shapes = [(length, PAIR)] * 5 + [(blocks, PAIR, PAIR)]
    local = pl.pallas_call(
        local_kernel,
        grid=(pairs,),
        in_specs=[wide] * 4 + [whole(rate), whole(surge), whole(docs)],
        out_specs=[part(2 * HEAD + 16, PAIR)] + [part(*s) for s in mid_shapes],
        out_shape=[sds((pairs, 2 * HEAD + 16, PAIR), BF16)]
        + [sds((pairs, *s), F32) for s in mid_shapes],
        cost_estimate=pl.CostEstimate(
            flops=6_000_000_000, bytes_accessed=6_000_000, transcendentals=600_000
        ),
        name="mixer_local",
        interpret=interpret,
    )
    pay, *mids = local(q, k, v, dec, rate, surge, docs)
    devices = lax.axis_size(("ring", "core"))
    pays = [
        lax.ppermute(pay, ("ring", "core"), [(d, (d + j) % devices) for d in range(devices)])
        for j in range(1, REACH + 1)
    ]
    outs = pl.pallas_call(
        outputs_kernel,
        grid=(pairs,),
        in_specs=[part(*s) for s in mid_shapes],
        out_specs=[part(length, PAIR)] * 2,
        out_shape=[sds((pairs, length, PAIR), F32)] * 2,
        cost_estimate=pl.CostEstimate(
            flops=5_000_000_000, bytes_accessed=6_000_000, transcendentals=0
        ),
        name="mixer_outputs",
        interpret=interpret,
    )(*mids)
    return pl.pallas_call(
        finish_kernel,
        out_shape=sds((length, weight.shape[1]), BF16),
        scratch_shapes=[pltpu.VMEM((length, width), BF16)],
        cost_estimate=pl.CostEstimate(
            flops=1_000_000_000, bytes_accessed=6_000_000, transcendentals=200_000
        ),
        name="mixer_finish",
        interpret=interpret,
    )(*outs, docs, scale.reshape(1, width), weight, *pays)


MESH = pl.DeviceIdType.MESH
QUARTERS = 4
MODEL = 2048
HALF = 128
UNIT = 256 + HALF


def pack_kernel(gate_ref, up_ref, down_ref, keep_ref, give_ref):
    core = lax.axis_index("core")
    for out_ref, half in ((keep_ref, core), (give_ref, 1 - core)):
        at = pl.ds(pl.multiple_of(half * HALF, HALF), HALF)
        for n in range(gate_ref.shape[1] // 256):
            rows = slice(n * 256, (n + 1) * 256)
            lanes = n * 256
            out_ref[0, :256, lanes : lanes + HALF] = gate_ref[0, rows, at]
            out_ref[0, :256, lanes + HALF : lanes + 256] = up_ref[0, rows, at]
        out_ref[0, 256:, :] = down_ref[0, at, :]


def pack(gate, up, down):
    steps = 4
    span = MODEL // steps
    tall = pl.BlockSpec((1, span, 256), lambda i, j: (i, j, 0))
    return pl.pallas_call(
        pack_kernel,
        grid=(EXP_DEV, steps),
        in_specs=[tall, tall, pl.BlockSpec((1, 256, span), lambda i, j: (i, 0, j))],
        out_specs=[pl.BlockSpec((1, UNIT, span), lambda i, j: (i, 0, j))] * 2,
        out_shape=[sds((EXP_DEV, UNIT, MODEL), BF16)] * 2,
        cost_estimate=pl.CostEstimate(
            flops=3_000_000_000, bytes_accessed=12_000_000, transcendentals=0
        ),
        name="pack_weights",
    )(gate, up, down)


def route_kernel(
    mixed_ref, residual_ref, scale_ref, routes_ref, weight_ref, stream_ref, out_ref, pick_ref
):
    rows = residual_ref.shape[0]
    z = residual_scale * residual_ref[...].astype(F32)
    for n in range(QUARTERS):
        z = z + mixed_ref[n].astype(F32)
    z = z - jnp.mean(z, -1, keepdims=True)
    spread_of = jnp.mean(z * z, -1, keepdims=True)
    stream = (z * lax.rsqrt(spread_of + norm_eps) * scale_ref[...]).astype(BF16)
    stream_ref[...] = stream
    start = pl.multiple_of(lax.axis_index("tp") * rows, rows)
    own = routes_ref[pl.ds(start, rows), :].astype(F32)
    entries = TOP * rows
    down = jnp.concatenate(
        [jnp.broadcast_to(own[:, k : k + 1], (rows, entries)) for k in range(TOP)], 0
    )
    earlier = iota(entries, entries, 1) < iota(entries, entries, 0)
    rank = jnp.sum(jnp.where((down == down.T) & earlier, 1.0, 0.0), -1, keepdims=True)
    slot = (2.0 * down[:, :1] + rank).astype(jnp.int32)
    slots = out_ref.shape[0]
    placed = (jnp.broadcast_to(slot, (entries, slots)) == iota(entries, slots, 1)).astype(F32)
    both = jnp.concatenate([stream] * TOP, 0)
    out_ref[...] = mm(placed.astype(BF16), both, TN).astype(BF16)
    pick = jnp.zeros((rows, slots), F32)
    for k in range(TOP):
        pick = pick + weight_ref[:, k : k + 1] * placed[k * rows : (k + 1) * rows]
    pick_ref[...] = pick


def route(mixed, residual, scale, routes, weight, slots):
    rows = residual.shape[0]
    return pl.pallas_call(
        route_kernel,
        out_shape=[
            sds((rows, MODEL), BF16),
            sds((slots, MODEL), BF16),
            sds((rows, slots), F32),
        ],
        cost_estimate=pl.CostEstimate(
            flops=1_000_000_000, bytes_accessed=3_000_000, transcendentals=0
        ),
        name="norm_route",
    )(mixed, residual, scale.reshape(1, MODEL), routes, weight)


def expert_kernel(rows_ref, *rest):
    count = (len(rest) - 3) // 2
    stored, out_ref, total = rest[:count], rest[count], rest[count + 1]
    parts, sems = rest[count + 2 : -1], rest[-1]
    rows = rows_ref.shape[0]
    loads = {}
    for n in range(count):
        loads[id(parts[n])] = pltpu.make_async_copy(stored[n], parts[n], sems.at[n])
        loads[id(parts[n])].start()
    units = [(p,) for p in parts if p.shape[1] == MODEL]
    cut = [p for p in parts if p.shape[1] < MODEL]
    units += list(zip(cut[::2], cut[1::2]))
    for n, unit in enumerate(units):
        wide = jnp.zeros((rows, 256), F32)
        begin = 0
        for w_ref in unit:
            loads[id(w_ref)].wait()
            for block in range(0, w_ref.shape[1], 256):
                part = w_ref[:256, block : block + 256]
                wide = wide + mm(rows_ref[:, begin + block : begin + block + 256], part)
            begin += w_ref.shape[1]
        gated, lifted = wide[:, :HALF], wide[:, HALF:]
        hidden = (gated / (1.0 + jnp.exp(-gated)) * lifted).astype(BF16)
        begin = 0
        for w_ref in unit:
            lanes = slice(begin, begin + w_ref.shape[1])
            part = mm(hidden, w_ref[256:, :])
            total[:, lanes] = part if n == 0 else total[:, lanes] + part
            begin += w_ref.shape[1]
    out_ref[...] = total[...].astype(BF16)


def expert(rows, units):
    return pl.pallas_call(
        expert_kernel,
        out_shape=sds(rows.shape, BF16),
        in_specs=[pl.BlockSpec(memory_space=pltpu.VMEM)]
        + [pl.BlockSpec(memory_space=pl.ANY)] * len(units),
        scratch_shapes=[pltpu.VMEM(rows.shape, F32)]
        + [pltpu.VMEM(u.shape, BF16) for u in units]
        + [pltpu.SemaphoreType.DMA((len(units),))],
        cost_estimate=pl.CostEstimate(
            flops=8_000_000_000, bytes_accessed=14_000_000, transcendentals=300_000
        ),
        name="expert_mlp",
    )(rows, *units)


def shared_kernel(rows_ref, gate_ref, up_ref, down_ref, out_ref):
    gated = mm(rows_ref[...], gate_ref[...])
    lifted = mm(rows_ref[...], up_ref[...])
    hidden = (gated / (1.0 + jnp.exp(-gated)) * lifted).astype(BF16)
    out_ref[...] = mm(hidden, down_ref[...]).astype(BF16)


def shared(rows, gate, up, down):
    return pl.pallas_call(
        shared_kernel,
        out_shape=sds(rows.shape, BF16),
        cost_estimate=pl.CostEstimate(
            flops=1_000_000_000, bytes_accessed=4_000_000, transcendentals=40_000
        ),
        name="shared_mlp",
    )(rows, gate, up, down)


def join_kernel(stream_ref, back_ref, pick_ref, shared_ref, out_ref):
    total = residual_scale * stream_ref[...].astype(F32)
    for n in range(QUARTERS):
        total = total + shared_ref[n].astype(F32)
    one, two = halves(pick_ref[...])
    out_ref[...] = (total + (mm(one, back_ref[...]) + mm(two, back_ref[...]))).astype(BF16)


def join(stream, back, pick, shared_rows):
    return pl.pallas_call(
        join_kernel,
        out_shape=sds(stream.shape, BF16),
        cost_estimate=pl.CostEstimate(
            flops=500_000_000, bytes_accessed=3_000_000, transcendentals=0
        ),
        name="join",
    )(stream, back, pick, shared_rows)


def exchange_kernel(out_ref, part_ref, in_ref, all_ref, sems):
    ring, core, quarter = (lax.axis_index(n) for n in ("ring", "core", "tp"))
    peers = out_ref.shape[0]
    me = ring * QUARTERS + quarter
    barrier = pltpu.get_barrier_semaphore()

    def place(n):
        return (n // QUARTERS, core, n % QUARTERS)

    def greet(n, carry):
        pl.semaphore_signal(
            barrier, inc=1, device_id=place((me + n) % peers), device_id_type=MESH
        )
        return carry

    lax.fori_loop(1, peers, greet, 0)
    own = [
        pltpu.make_async_copy(out_ref.at[me], in_ref.at[me], sems.at[4]),
        pltpu.make_async_copy(
            part_ref.at[quarter % part_ref.shape[0]], all_ref.at[quarter], sems.at[5]
        ),
    ]
    for copy in own:
        copy.start()
    pl.semaphore_wait(barrier, peers - 1)

    def send(to):
        return pltpu.make_async_remote_copy(
            src_ref=out_ref.at[to],
            dst_ref=in_ref.at[me],
            send_sem=sems.at[0],
            recv_sem=sems.at[1],
            device_id=place(to),
            device_id_type=MESH,
        )

    def pair(n, carry):
        send((me + n) % peers).start()
        send((me + peers - n) % peers).start()
        return carry

    def mate(n):
        to = (quarter + n) % QUARTERS
        return pltpu.make_async_remote_copy(
            src_ref=part_ref.at[to % part_ref.shape[0]],
            dst_ref=all_ref.at[quarter],
            send_sem=sems.at[2],
            recv_sem=sems.at[3],
            device_id=(ring, core, to),
            device_id_type=MESH,
        )

    send((me + peers // 2) % peers).start()
    for n in (2, 1, 3):
        mate(n).start()
    lax.fori_loop(1, peers // 2, pair, 0)
    for copy in own:
        copy.wait()
    some = slice(0, QUARTERS - 1)
    mates = pltpu.make_async_remote_copy(
        src_ref=all_ref.at[some],
        dst_ref=all_ref.at[some],
        send_sem=sems.at[2],
        recv_sem=sems.at[3],
        device_id=(ring, core, (quarter + 1) % QUARTERS),
        device_id_type=MESH,
    )
    most = slice(0, peers - 1)
    blocks = pltpu.make_async_remote_copy(
        src_ref=out_ref.at[most],
        dst_ref=in_ref.at[most],
        send_sem=sems.at[0],
        recv_sem=sems.at[1],
        device_id=place((me + 1) % peers),
        device_id_type=MESH,
    )
    for copy in (mates, blocks):
        copy.wait_send()
        copy.wait_recv()


def exchange(blocks, part, name, number):
    rows = part.shape[1]
    return pl.pallas_call(
        exchange_kernel,
        in_specs=[pl.BlockSpec(memory_space=pltpu.VMEM)] * 2,
        out_specs=[pl.BlockSpec(memory_space=pltpu.VMEM)] * 2,
        out_shape=[sds(blocks.shape, BF16), sds((QUARTERS, rows, MODEL), BF16)],
        scratch_shapes=[pltpu.SemaphoreType.DMA((6,))],
        compiler_params=pltpu.CompilerParams(collective_id=number, has_side_effects=True),
        cost_estimate=pl.CostEstimate(
            flops=15_000_000_000, bytes_accessed=4_000_000, transcendentals=0
        ),
        name=name,
    )(blocks, part)


def swap_cores(x):
    return lax.ppermute(x, "core", [(0, 1), (1, 0)])


def shifted(x, shift):
    return lax.ppermute(x, "tp", [(n, (n + shift) % QUARTERS) for n in range(QUARTERS)])


def by_quarter(x, axis):
    return lax.all_to_all(x, axis, split_axis=0, concat_axis=0, tiled=True)


def per_device(
    head_queries,
    head_keys,
    head_values,
    decay_logits,
    learning_logits,
    surge_decay,
    documents,
    residual,
    head_norm_scale,
    mixer_output_weight,
    layer_norm_scale,
    routes,
    routing_weight,
    routed_gate_weight,
    routed_up_weight,
    routed_down_weight,
    common_gate_weight,
    common_up_weight,
    common_down_weight,
):
    rows = residual.shape[0]
    keep, give = pack(routed_gate_weight, routed_up_weight, routed_down_weight)
    other = swap_cores(give)
    core, quarter = lax.axis_index("core"), lax.axis_index("tp")

    def share(shift):
        target = (quarter + shift) & (QUARTERS - 1)
        odd = (target & 1) == 1
        kept, swapped = (jnp.where(odd, x[1], x[0]) for x in (keep, other))
        return jnp.where((target >> 1) == core, kept, swapped)

    far = share(2)
    near = [share(0), shifted(share(1), 1), shifted(share(3), 3)]
    hops = [shifted(far[:, :1024], 1), shifted(far[:, 1024:], 3)]
    mixed = mixer(
        head_queries,
        head_keys,
        head_values,
        decay_logits,
        learning_logits,
        surge_decay,
        documents,
        head_norm_scale,
        mixer_output_weight,
    )
    near, hops, mixed = lax.optimization_barrier((near, hops, mixed))
    far = [shifted(hops[0], 1), shifted(hops[1], 3)]
    parts = [*near, *(swap_cores(x) for x in near), *far, *(swap_cores(x) for x in far)]
    slots = lax.axis_size(("ring", "tp")) * 2
    arrived = by_quarter(mixed.reshape(QUARTERS, rows, MODEL), "tp")
    stream, outgoing, pick = route(
        arrived, residual, layer_norm_scale, routes, routing_weight, slots
    )
    blocks = (slots // 2, 2, MODEL)
    incoming, rows_all = exchange(outgoing.reshape(blocks), stream[None], "dispatch", 1)
    shared_part = shared(
        rows_all.reshape(-1, MODEL), common_gate_weight, common_up_weight, common_down_weight
    )
    answers = expert(incoming.reshape(slots, MODEL), parts)
    back, shared_rows = exchange(
        answers.reshape(blocks), shared_part.reshape(QUARTERS, rows, MODEL), "giveback", 2
    )
    return join(stream, back.reshape(slots, MODEL), pick, shared_rows)


def solution(mesh):
    torus = Mesh(mesh.devices.reshape(-1, 2, QUARTERS), ("ring", "core", "tp"))
    sp = ("ring", "core")
    rows = P(sp, "tp")
    own = P((*sp, "tp"), None)
    placed = (
        *(rows,) * 6,
        P(sp),
        own,
        P("tp"),
        P("tp", None),
        P(),
        P(sp, None),
        own,
        P(sp, None, "tp"),
        P(sp, None, "tp"),
        P(sp, "tp", None),
        P(None, "tp"),
        P(None, "tp"),
        P("tp", None),
    )
    return jax.shard_map(
        per_device, mesh=torus, in_specs=placed, out_specs=own, check_vma=False
    )
```

```python
import itertools
import jax
import jax.numpy as jnp
from jax import lax
from jax.experimental import pallas as pl
from jax.experimental.pallas import tpu as pltpu
from jax.sharding import Mesh
from jax.sharding import PartitionSpec as P

MESH = pl.DeviceIdType.MESH
QUARTERS = 4
MODEL = 2048
DEEP = 1024
HALF = 128
HEAD = 64
PAIR = 128
SPAN = 64
REACH = 6
EXP_DEV = 2
TOP = 2
TOK_DEV = 64

residual_scale = 2.0**0.5
group_eps = 0.00064
norm_eps = 1e-05
unit_eps = 1e-06
F32, BF16 = jnp.float32, jnp.bfloat16

NN = (((1,), (0,)), ((), ()))
NT = (((1,), (1,)), ((), ()))
TN = (((0,), (0,)), ((), ()))


def iota(rows, cols, axis):
    return lax.broadcasted_iota(jnp.int32, (rows, cols), axis)


def mm(a, b, dims=NN):
    return lax.dot_general(a, b, dims, preferred_element_type=F32)


def halves(x):
    high = x.astype(BF16)
    return high, (x - high.astype(F32)).astype(BF16)


def thirds(x):
    high = x.astype(BF16)
    rest = x - high.astype(F32)
    mid = rest.astype(BF16)
    return high, mid, (rest - mid.astype(F32)).astype(BF16)


def mm3(a, b, dims=NN):
    return mm(a[0], b[0], dims) + (mm(a[1], b[0], dims) + mm(a[0], b[1], dims))


def exact_right(a, b):
    one, two, three = thirds(b)
    return mm(a, one) + (mm(a, two) + mm(a, three))


def head_masks():
    lane = iota(1, PAIR, 1)
    return (lane < HEAD).astype(F32).astype(BF16), (lane >= HEAD).astype(F32).astype(BF16)


def spread_one(x, masks):
    return jnp.concatenate([x * masks[0], x * masks[1]], axis=0)


def spread(pair, masks):
    return tuple(spread_one(x, masks) for x in pair)


def beside(a, b, axis):
    return tuple(jnp.concatenate([x, y], axis=axis) for x, y in zip(a, b))


def greet_ring(barrier):
    ring, core, quarter = (lax.axis_index(n) for n in ("ring", "core", "tp"))
    for n in range(1, 2 * QUARTERS):
        at = (core * QUARTERS + quarter + n) % (2 * QUARTERS)
        pl.semaphore_signal(
            barrier,
            inc=1,
            device_id=(ring, at // QUARTERS, at % QUARTERS),
            device_id_type=MESH,
        )


def remote(src, dst, send, recv, device):
    return pltpu.make_async_remote_copy(
        src_ref=src,
        dst_ref=dst,
        send_sem=send,
        recv_sem=recv,
        device_id=device,
        device_id_type=MESH,
    )


def weight_views(gate_ref, up_ref, down_ref, which, half):
    return (
        gate_ref.at[which, pl.ds(half * DEEP, DEEP)],
        up_ref.at[which, pl.ds(half * DEEP, DEEP)],
        down_ref.at[which, pl.ds(half * HALF, HALF)],
    )


def send_shift(shift, weights, stage, targets, send, recv, part):
    ring, core, quarter = (lax.axis_index(n) for n in ("ring", "core", "tp"))
    goal = (quarter + shift) % QUARTERS
    which = goal % EXP_DEV
    owned = goal // EXP_DEV == core

    def copies(sources):
        return [
            remote(src, dst, send.at[n], recv.at[n], (ring, core, goal))
            for n, (src, dst) in enumerate(zip(sources, targets))
        ]

    if part == "wait":
        for copy in copies(targets):
            copy.wait_send()
            copy.wait_recv()
        return

    @pl.when(owned if part == "own" else goal // EXP_DEV != core)
    def _():
        held = [ref.at[which] for ref in stage]
        for copy in copies(weight_views(*weights, which, core) if part == "own" else held):
            copy.start()


def local_kernel(
    q_ref, k_ref, v_ref, dec_ref, rate_ref, surge_ref, doc_ref, gate_ref, up_ref, down_ref,
    pay_ref, ru_ref, rkv_ref, cm_ref, lp_ref, fj_ref, state_ref,
    g_ref, u_ref, d_ref, g_stage_ref, u_stage_ref, d_stage_ref,
    send, recv, stage_send, stage_recv,
):
    ring, core, quarter = (lax.axis_index(n) for n in ("ring", "core", "tp"))
    weights = (gate_ref, up_ref, down_ref)
    stage = (g_stage_ref, u_stage_ref, d_stage_ref)
    near = (g_ref, u_ref, d_ref)
    mate = (ring, 1 - core, quarter)

    def staged(turn):
        which = (quarter + 1 + turn) % EXP_DEV
        sources = weight_views(*weights, which, 1 - core)
        return [
            remote(src, dst.at[which], stage_send.at[turn, n], stage_recv.at[turn, n], mate)
            for n, (src, dst) in enumerate(zip(sources, stage))
        ]

    def moves(part):
        for unit, shift in enumerate((1, 3)):
            targets = [ref.at[unit] for ref in near]
            send_shift(shift, weights, stage, targets, send.at[unit], recv.at[unit], part)

    @pl.when(pl.program_id(0) == 0)
    def _():
        barrier = pltpu.get_barrier_semaphore()
        greet_ring(barrier)
        pl.semaphore_wait(barrier, 2 * QUARTERS - 1)
        for copy in staged(0):
            copy.start()
        moves("own")

    def pause():
        @pl.when(pl.program_id(0) == 0)
        def _():
            for copy in staged(0):
                copy.wait_recv()
            moves("mate")
            for copy in staged(1):
                copy.start()

    local_body(
        q_ref, k_ref, v_ref, dec_ref, rate_ref, surge_ref, doc_ref,
        pay_ref, ru_ref, rkv_ref, cm_ref, lp_ref, fj_ref, state_ref, pause,
    )

    @pl.when(pl.program_id(0) == pl.num_programs(0) - 1)
    def _():
        for copy in staged(0):
            copy.wait_send()
        for copy in staged(1):
            copy.wait_send()
            copy.wait_recv()
        moves("wait")


def local_body(
    q_ref, k_ref, v_ref, dec_ref, rate_ref, surge_ref, doc_ref,
    pay_ref, ru_ref, rkv_ref, cm_ref, lp_ref, fj_ref, state_ref, pause,
):
    pair = pl.program_id(0)
    length = q_ref.shape[0]
    blocks = length // SPAN
    masks = head_masks()
    head_same = iota(PAIR, PAIR, 0) // HEAD == iota(PAIR, PAIR, 1) // HEAD
    queries, keys, values = (r[...].astype(F32) for r in (q_ref, k_ref, v_ref))
    chosen = (iota(8, PAIR, 0) == 2 * pair + iota(8, PAIR, 1) // HEAD).astype(F32)
    rates = 1.0 / (1.0 + jnp.exp(-rate_ref[...].astype(F32)))
    rate = jnp.dot(rates, chosen, precision=lax.Precision.HIGHEST, preferred_element_type=F32)
    surge = jnp.dot(
        surge_ref[...], chosen, precision=lax.Precision.HIGHEST, preferred_element_type=F32
    )
    same = head_same.astype(F32).astype(BF16)
    one, two = halves(keys * keys)
    unit = keys * lax.rsqrt(mm(one, same) + mm(two, same) + unit_eps)
    decay = surge - 0.6065306597126334 / (1.0 + jnp.exp(-dec_ref[...].astype(F32)))
    row, col = iota(length, length, 0), iota(length, length, 1)
    lower = ((row // SPAN == col // SPAN) & (col <= row)).astype(F32).astype(BF16)
    cumulative = exact_right(lower, decay)
    back, ahead = jnp.exp(-cumulative), jnp.exp(cumulative - decay)
    ahead_unit = unit * ahead
    back_unit = unit * rate * back
    back_key = keys * back
    forward = queries * jnp.exp(cumulative)
    docs_row = doc_ref[...].astype(F32)
    diagonal = jnp.where(row == col, jnp.broadcast_to(docs_row, (length, length)), 0.0)
    docs = mm(diagonal.astype(BF16), jnp.ones((length, PAIR), BF16))
    pick = (iota(SPAN, PAIR, 1) == 0).astype(F32).astype(BF16)
    t_pos, s_pos = iota(SPAN, PAIR, 0), iota(SPAN, PAIR, 1) % HEAD
    eye = (t_pos == s_pos).astype(F32)
    big_eye = iota(PAIR, PAIR, 0) == iota(PAIR, PAIR, 1)
    carried = through = None
    for b in range(blocks):
        if b == 1:
            pause()
        at = slice(b * SPAN, (b + 1) * SPAN)
        doc = docs[at]
        prior = docs[max(b * SPAN - 1, 0) : max(b * SPAN - 1, 0) + 1]
        joined = (doc == prior).astype(F32)
        tail = (doc == doc[SPAN - 1 :]).astype(F32)
        doc16 = doc.astype(BF16)
        doc_s = mm(pick, jnp.concatenate([doc16, doc16], 0), NT)
        same_doc = doc == doc_s
        strict = same_doc & (t_pos > s_pos)
        causal = same_doc & (t_pos >= s_pos)
        left = halves(jnp.concatenate([ahead_unit[at], forward[at]], 0))
        right = beside(
            spread(halves(back_unit[at]), masks), spread(halves(back_key[at]), masks), 0
        )
        scores = mm3(left, right, NT)
        inner = jnp.where(strict, scores[:SPAN, :PAIR], 0.0)
        mix_key = jnp.where(strict, scores[:SPAN, PAIR:], 0.0)
        read_unit = jnp.where(causal, -scores[SPAN:, :PAIR], 0.0)
        read_key = jnp.where(causal, scores[SPAN:, PAIR:], 0.0)
        near = jnp.where(t_pos // 16 == s_pos // 16, inner, 0.0)
        x = eye - near
        n_pair = halves(near)
        power = mm3(n_pair, spread(n_pair, masks))
        for step in range(3):
            p_pair = halves(power)
            p_wide = spread(p_pair, masks)
            if step < 2:
                both = mm3(beside(halves(x), p_pair, 0), p_wide)
                x, power = x + both[:SPAN], both[SPAN:]
            else:
                x = x + mm3(halves(x), p_wide)
        for width in (32, 64):
            cross = (t_pos // width == s_pos // width) & (
                t_pos // (width // 2) != s_pos // (width // 2)
            )
            part = spread(halves(jnp.where(cross, inner, 0.0)), masks)
            x_pair = halves(x)
            x = x - mm3(halves(mm3(x_pair, part)), spread(x_pair, masks))
        value = values[at].astype(BF16)
        value_wide = spread_one(value, masks)
        weights = halves(jnp.concatenate([mix_key, read_key], 0))
        weighed = mm(weights[0], value_wide) + mm(weights[1], value_wide)
        rkv_ref[0, at] = weighed[SPAN:]
        side = beside(
            spread(halves(ahead_unit[at] * joined), masks),
            spread(halves(weighed[:SPAN]), masks),
            1,
        )
        solved = mm3(halves(x), side)
        carry_map, local_pull = solved[:, :PAIR], solved[:, PAIR:]
        ru_ref[0, at] = read_unit
        cm_ref[0, at] = carry_map
        lp_ref[0, at] = local_pull
        fj_ref[0, at] = forward[at] * joined
        total = cumulative[b * SPAN + SPAN - 1 : b * SPAN + SPAN]
        to_end = jnp.exp(total - cumulative[at]) * tail
        end_unit = halves(unit[at] * (to_end * -rate[at]))
        end_key = halves(keys[at] * to_end)
        block_map = mm3(halves(carry_map), end_unit, TN)
        block_map = jnp.where(head_same, block_map, 0.0) + jnp.where(
            big_eye, jnp.exp(total) * joined[SPAN - 1 :], 0.0
        )
        add = mm3(halves(local_pull), end_unit, TN) + (
            mm(value, end_key[0], TN) + mm(value, end_key[1], TN)
        )
        add = jnp.where(head_same, add, 0.0)
        add = add[:HEAD] + add[HEAD:]
        if b == 0:
            state_ref[0, 0] = jnp.concatenate([jnp.zeros((HEAD, PAIR), F32), eye], 0)
            carried, through = add, block_map[:HEAD] + block_map[HEAD:]
        else:
            before = jnp.concatenate([carried, through], 0)
            state_ref[0, b] = before
            after = mm3(halves(before), halves(block_map))
            carried, through = after[:HEAD] + add, after[HEAD:]
    pay_ref[0, :HEAD] = through.astype(BF16)
    pay_ref[0, HEAD : 2 * HEAD] = carried.astype(BF16)
    pay_ref[0, 2 * HEAD :] = jnp.broadcast_to(docs[length - 1 :], (16, PAIR)).astype(BF16)


def tail_kernel(
    pay_ref, ru_ref, rkv_ref, cm_ref, lp_ref, fj_ref, state_ref, doc_ref, head_scale_ref, w_ref,
    residual_ref, scale_ref, routes_ref, weight_ref, gate_ref, up_ref, down_ref,
    g_ref, u_ref, d_ref, g_stage_ref, u_stage_ref, d_stage_ref,
    stream_ref, slots_ref, pick_ref, g_swap_ref, u_swap_ref, d_swap_ref,
    g_zero_ref, u_zero_ref, d_zero_ref, g_far_ref, u_far_ref, d_far_ref,
    out_ref, start_ref, heads, pays, mixed, mixed_in,
    pay_send, pay_recv, swap_send, swap_recv, zero_send, zero_recv, far_send, far_recv,
    tp_send, tp_recv,
):
    ring, core, quarter = (lax.axis_index(n) for n in ("ring", "core", "tp"))
    place = 2 * ring + core
    devices = 2 * lax.axis_size("ring")
    barrier = pltpu.get_barrier_semaphore()
    greet_ring(barrier)

    def along(n):
        at = (place + n) % devices
        return (at // 2, at % 2, quarter)

    for j in range(1, REACH + 1):
        pl.semaphore_signal(
            barrier, inc=1, device_id=along(devices - j), device_id_type=MESH
        )
    pl.semaphore_wait(barrier, REACH + 2 * QUARTERS - 1)
    sends = [
        remote(pay_ref, pays.at[j - 1], pay_send.at[j - 1], pay_recv.at[j - 1], along(j))
        for j in range(REACH, 0, -1)
    ]
    mate = (ring, 1 - core, quarter)
    swaps = [
        remote(src, dst, swap_send.at[n], swap_recv.at[n], mate)
        for n, (src, dst) in enumerate(
            ((g_ref, g_swap_ref), (u_ref, u_swap_ref), (d_ref, d_swap_ref))
        )
    ]
    weights = (gate_ref, up_ref, down_ref)
    stage = (g_stage_ref, u_stage_ref, d_stage_ref)
    far = (weights, stage, (g_far_ref, u_far_ref, d_far_ref), far_send, far_recv)
    zero = (g_zero_ref, u_zero_ref, d_zero_ref)
    which = quarter % EXP_DEV

    def zeros(sources):
        return [
            remote(src, dst, zero_send.at[n], zero_recv.at[n], mate)
            for n, (src, dst) in enumerate(zip(sources, zero))
        ]

    for copy in sends:
        copy.start()
    for part in ("own", "mate"):
        send_shift(2, *far, part)
    for copy in swaps:
        copy.start()

    @pl.when(quarter // EXP_DEV == core)
    def _():
        for copy in zeros(weight_views(*weights, which, core)):
            copy.start()

    @pl.when(quarter // EXP_DEV != core)
    def _():
        for copy in zeros([ref.at[which] for ref in stage]):
            copy.start()

    outputs_body(ru_ref, rkv_ref, cm_ref, lp_ref, fj_ref, state_ref, out_ref, start_ref)
    for copy in sends:
        copy.wait_recv()
    finish_body(out_ref, start_ref, doc_ref, head_scale_ref, pays, heads)
    rows = residual_ref.shape[0]
    trips = []
    for n in (2, 1, 3):
        to = (quarter + n) % QUARTERS
        at = pl.ds(pl.multiple_of(to * rows, rows), rows)
        mixed[n] = mm(heads[at, :], w_ref[...]).astype(BF16)
        trips.append(
            remote(
                mixed.at[n],
                mixed_in.at[n],
                tp_send.at[n - 1],
                tp_recv.at[n - 1],
                (ring, core, to),
            )
        )
        trips[-1].start()
    at = pl.ds(pl.multiple_of(quarter * rows, rows), rows)
    mixed_in[0] = mm(heads[at, :], w_ref[...]).astype(BF16)
    for copy in trips:
        copy.wait_recv()
    route_kernel(
        mixed_in, residual_ref, scale_ref, routes_ref, weight_ref, stream_ref, slots_ref, pick_ref
    )
    for copy in sends + trips:
        copy.wait_send()
    for copy in swaps + zeros(zero):
        copy.wait_send()
        copy.wait_recv()
    send_shift(2, *far, "wait")


def outputs_body(ru_ref, rkv_ref, cm_ref, lp_ref, fj_ref, state_ref, out_ref, start_ref):
    masks = head_masks()
    for pair, b in itertools.product(range(ru_ref.shape[0]), range(ru_ref.shape[1] // SPAN)):
        at = slice(b * SPAN, (b + 1) * SPAN)
        side = beside(
            spread(halves(cm_ref[pair, at]), masks), spread(halves(lp_ref[pair, at]), masks), 1
        )
        z = mm3(halves(ru_ref[pair, at]), side)
        begin = halves(fj_ref[pair, at] + z[:, :PAIR])
        states = halves(state_ref[pair, b])
        wide = beside(
            spread(tuple(s[:HEAD] for s in states), masks),
            spread(tuple(s[HEAD:] for s in states), masks),
            0,
        )
        y = mm3(begin, wide, NT)
        out_ref[pair, at] = rkv_ref[pair, at] + z[:, PAIR:] + y[:, :PAIR]
        start_ref[pair, at] = y[:, PAIR:]


def finish_body(out_ref, start_ref, doc_ref, scale_ref, pays, heads):
    masks = head_masks()
    same = (iota(PAIR, PAIR, 0) // HEAD == iota(PAIR, PAIR, 1) // HEAD).astype(F32)
    same = (same * (1.0 / HEAD)).astype(BF16)
    first = jnp.broadcast_to(doc_ref[:, :1].astype(F32), (1, PAIR))

    def mean(x):
        one, two = halves(x)
        return mm(one, same) + mm(two, same)

    for pair in range(out_ref.shape[0]):
        state = None
        for j in range(REACH - 1, -1, -1):
            pay = pays.at[j]
            linked = pay[pair, 2 * HEAD : 2 * HEAD + 1].astype(F32) == first
            add = pay[pair, HEAD : 2 * HEAD].astype(F32)
            if state is not None:
                wide = spread_one(pay[pair, :HEAD], masks)
                one, two = halves(state)
                add = add + (mm(one, wide) + mm(two, wide))
            state = jnp.where(linked, add, 0.0)
        wide = spread(halves(state), masks)
        read = out_ref[pair] + mm3(halves(start_ref[pair]), wide, NT)
        centred = read - mean(read)
        normed = centred * lax.rsqrt(mean(centred * centred) + group_eps)
        lanes = slice(pair * PAIR, (pair + 1) * PAIR)
        heads[:, lanes] = (normed * scale_ref[:, lanes]).astype(BF16)


def sds(shape, dtype):
    return jax.ShapeDtypeStruct(shape, dtype)


def mixer(q, k, v, dec, rate, surge, documents, scale, weight, rest, routed):
    length, width = q.shape
    pairs = width // PAIR
    blocks = length // SPAN
    docs = documents.reshape(1, length)
    residual, norm_scale, routes, routing_weight = rest
    rows = residual.shape[0]
    slots = 2 * QUARTERS * lax.axis_size("ring")
    wide = pl.BlockSpec((length, PAIR), lambda p: (0, p))
    whole = lambda a: pl.BlockSpec(a.shape, lambda p: (0,) * a.ndim)
    part = lambda *dims: pl.BlockSpec((1, *dims), lambda p: (p,) + (0,) * len(dims))
    stored = pl.BlockSpec(memory_space=pl.ANY)
    inside = pl.BlockSpec(memory_space=pltpu.VMEM)
    semaphores = pltpu.SemaphoreType.DMA
    mid_shapes = [(length, PAIR)] * 5 + [(blocks, PAIR, PAIR)]
    *mids, near_g, near_u, near_d, stage_g, stage_u, stage_d = pl.pallas_call(
        local_kernel,
        grid=(pairs,),
        in_specs=[wide] * 4 + [whole(rate), whole(surge), whole(docs)] + [stored] * 3,
        out_specs=[part(2 * HEAD + 16, PAIR)] + [part(*s) for s in mid_shapes] + [stored] * 6,
        out_shape=[sds((pairs, 2 * HEAD + 16, PAIR), BF16)]
        + [sds((pairs, *s), F32) for s in mid_shapes]
        + ([sds((2, DEEP, 2 * HALF), BF16)] * 2 + [sds((2, HALF, MODEL), BF16)]) * 2,
        scratch_shapes=[semaphores((2, 3))] * 4,
        compiler_params=pltpu.CompilerParams(collective_id=3, has_side_effects=True),
        cost_estimate=pl.CostEstimate(
            flops=6_000_000_000, bytes_accessed=6_000_000, transcendentals=600_000
        ),
        name="mixer_local",
    )(q, k, v, dec, rate, surge, docs, *routed)
    return (near_g, near_u, near_d), (stage_g, stage_u, stage_d), pl.pallas_call(
        tail_kernel,
        in_specs=[inside] * 14 + [stored] * 9,
        out_specs=[inside] * 3 + [stored] * 9,
        out_shape=[
            sds((rows, MODEL), BF16),
            sds((slots, MODEL), BF16),
            sds((rows, slots), F32),
            sds(near_g.shape, BF16),
            sds(near_u.shape, BF16),
            sds(near_d.shape, BF16),
            sds((DEEP, 2 * HALF), BF16),
            sds((DEEP, 2 * HALF), BF16),
            sds((HALF, MODEL), BF16),
            sds((DEEP, 2 * HALF), BF16),
            sds((DEEP, 2 * HALF), BF16),
            sds((HALF, MODEL), BF16),
        ],
        scratch_shapes=[
            pltpu.VMEM((pairs, length, PAIR), F32),
            pltpu.VMEM((pairs, length, PAIR), F32),
            pltpu.VMEM((length, width), BF16),
            pltpu.VMEM((REACH, pairs, 2 * HEAD + 16, PAIR), BF16),
            pltpu.VMEM((QUARTERS, rows, MODEL), BF16),
            pltpu.VMEM((QUARTERS, rows, MODEL), BF16),
            semaphores((REACH,)),
            semaphores((REACH,)),
            semaphores((3,)),
            semaphores((3,)),
            semaphores((3,)),
            semaphores((3,)),
            semaphores((3,)),
            semaphores((3,)),
            semaphores((QUARTERS - 1,)),
            semaphores((QUARTERS - 1,)),
        ],
        compiler_params=pltpu.CompilerParams(collective_id=4, has_side_effects=True),
        cost_estimate=pl.CostEstimate(
            flops=6_000_000_000, bytes_accessed=12_000_000, transcendentals=200_000
        ),
        name="mixer_tail",
    )(
        *mids,
        docs,
        scale.reshape(1, width),
        weight,
        residual,
        norm_scale.reshape(1, MODEL),
        routes,
        routing_weight,
        *routed,
        near_g,
        near_u,
        near_d,
        stage_g,
        stage_u,
        stage_d,
    )


def route_kernel(
    mixed_ref, residual_ref, scale_ref, routes_ref, weight_ref, stream_ref, out_ref, pick_ref
):
    rows = residual_ref.shape[0]
    z = residual_scale * residual_ref[...].astype(F32)
    for n in range(QUARTERS):
        z = z + mixed_ref[n].astype(F32)
    z = z - jnp.mean(z, -1, keepdims=True)
    spread_of = jnp.mean(z * z, -1, keepdims=True)
    stream = (z * lax.rsqrt(spread_of + norm_eps) * scale_ref[...]).astype(BF16)
    stream_ref[...] = stream
    start = pl.multiple_of(lax.axis_index("tp") * rows, rows)
    own = routes_ref[pl.ds(start, rows), :].astype(F32)
    entries = TOP * rows
    down = jnp.concatenate(
        [jnp.broadcast_to(own[:, k : k + 1], (rows, entries)) for k in range(TOP)], 0
    )
    earlier = iota(entries, entries, 1) < iota(entries, entries, 0)
    rank = jnp.sum(jnp.where((down == down.T) & earlier, 1.0, 0.0), -1, keepdims=True)
    slot = (2.0 * down[:, :1] + rank).astype(jnp.int32)
    slots = out_ref.shape[0]
    placed = (jnp.broadcast_to(slot, (entries, slots)) == iota(entries, slots, 1)).astype(F32)
    both = jnp.concatenate([stream] * TOP, 0)
    out_ref[...] = mm(placed.astype(BF16), both, TN).astype(BF16)
    pick = jnp.zeros((rows, slots), F32)
    for k in range(TOP):
        pick = pick + weight_ref[:, k : k + 1] * placed[k * rows : (k + 1) * rows]
    pick_ref[...] = pick


def expert_kernel(rows_ref, gate_ref, up_ref, down_ref, *rest):
    count = (len(rest) - 3) // 2
    stored, out_ref, total = rest[:count], rest[count], rest[count + 1]
    held, sems = rest[count + 2 : -1], rest[-1]
    core, quarter = lax.axis_index("core"), lax.axis_index("tp")
    which = quarter % EXP_DEV
    first_own = weight_views(gate_ref, up_ref, down_ref, which, core)
    loads = []

    def load(src, dst, other=None):
        at = sems.at[len(loads)]
        copy = pltpu.make_async_copy(src, dst, at)
        loads.append(copy)
        if other is None:
            copy.start()
        else:
            pl.when(quarter // EXP_DEV == core)(pltpu.make_async_copy(other, dst, at).start)
            pl.when(quarter // EXP_DEV != core)(copy.start)
        return copy, dst

    units = [
        [load(stored[k].at[which], held[k].at[0], first_own[k]) for k in range(3)]
        + [load(stored[3 + k].at[0], held[3 + k].at[0]) for k in range(3)]
    ]
    for at in range(6, count, 6):
        for n in range(stored[at].shape[0]):
            units.append([load(stored[at + k].at[n], held[at + k].at[n]) for k in range(6)])

    def ready(item):
        item[0].wait()
        return item[1][...]

    first = core == 0
    own = rows_ref[:, pl.ds(pl.multiple_of(core * DEEP, DEEP), DEEP)]
    rest_of = rows_ref[:, pl.ds(pl.multiple_of((1 - core) * DEEP, DEEP), DEEP)]
    for n, (gate, up, down, gate_two, up_two, down_two) in enumerate(units):
        gated = mm(own, ready(gate)) + mm(rest_of, ready(gate_two))
        lifted = mm(own, ready(up)) + mm(rest_of, ready(up_two))
        hidden = gated / (1.0 + jnp.exp(-gated)) * lifted
        low, high = hidden[:, :HALF], hidden[:, HALF:]
        part = mm(jnp.where(first, low, high).astype(BF16), ready(down)) + mm(
            jnp.where(first, high, low).astype(BF16), ready(down_two)
        )
        total[...] = part if n == 0 else total[...] + part
    out_ref[...] = total[...].astype(BF16)


def expert(rows, raw, weights):
    held = [(1, *w.shape[1:]) for w in weights[:3]] + [w.shape for w in weights[3:]]
    count = sum(h[0] for h in held)
    return pl.pallas_call(
        expert_kernel,
        in_specs=[pl.BlockSpec(memory_space=pltpu.VMEM)]
        + [pl.BlockSpec(memory_space=pl.ANY)] * (3 + len(weights)),
        out_shape=sds(rows.shape, BF16),
        scratch_shapes=[pltpu.VMEM(rows.shape, F32)]
        + [pltpu.VMEM(h, BF16) for h in held]
        + [pltpu.SemaphoreType.DMA((count,))],
        cost_estimate=pl.CostEstimate(
            flops=8_000_000_000, bytes_accessed=14_000_000, transcendentals=300_000
        ),
        name="expert_mlp",
    )(rows, *raw, *weights)


def shared_kernel(rows_ref, gate_ref, up_ref, down_ref, out_ref):
    gated = mm(rows_ref[...], gate_ref[...])
    lifted = mm(rows_ref[...], up_ref[...])
    hidden = (gated / (1.0 + jnp.exp(-gated)) * lifted).astype(BF16)
    out_ref[...] = mm(hidden, down_ref[...]).astype(BF16)


def shared(rows, gate, up, down):
    return pl.pallas_call(
        shared_kernel,
        out_shape=sds(rows.shape, BF16),
        cost_estimate=pl.CostEstimate(
            flops=1_000_000_000, bytes_accessed=4_000_000, transcendentals=40_000
        ),
        name="shared_mlp",
    )(rows, gate, up, down)


def join_kernel(stream_ref, back_ref, pick_ref, shared_ref, out_ref):
    total = residual_scale * stream_ref[...].astype(F32)
    for n in range(QUARTERS):
        total = total + shared_ref[n].astype(F32)
    one, two = halves(pick_ref[...])
    out_ref[...] = (total + (mm(one, back_ref[...]) + mm(two, back_ref[...]))).astype(BF16)


def join(stream, back, pick, shared_rows):
    return pl.pallas_call(
        join_kernel,
        out_shape=sds(stream.shape, BF16),
        cost_estimate=pl.CostEstimate(
            flops=500_000_000, bytes_accessed=3_000_000, transcendentals=0
        ),
        name="join",
    )(stream, back, pick, shared_rows)


def exchange_kernel(*refs):
    swapping = len(refs) > 5
    out_ref, part_ref, *rest = refs
    if swapping:
        weights, (in_ref, all_ref), swapped, sems = rest[:3], rest[3:5], rest[5:8], rest[8]
    else:
        in_ref, all_ref, sems = rest
    ring, core, quarter = (lax.axis_index(n) for n in ("ring", "core", "tp"))
    peers = out_ref.shape[0]
    me = ring * QUARTERS + quarter
    barrier = pltpu.get_barrier_semaphore()

    def place(n):
        return (n // QUARTERS, core, n % QUARTERS)

    def greet(n, carry):
        pl.semaphore_signal(
            barrier, inc=1, device_id=place((me + n) % peers), device_id_type=MESH
        )
        return carry

    lax.fori_loop(1, peers, greet, 0)
    mate_core = (ring, 1 - core, quarter)
    if swapping:
        pl.semaphore_signal(barrier, inc=1, device_id=mate_core, device_id_type=MESH)
    own = [
        pltpu.make_async_copy(out_ref.at[me], in_ref.at[me], sems.at[4]),
        pltpu.make_async_copy(
            part_ref.at[quarter % part_ref.shape[0]], all_ref.at[quarter], sems.at[5]
        ),
    ]
    for copy in own:
        copy.start()
    pl.semaphore_wait(barrier, peers - 1 + swapping)

    def send(to):
        return pltpu.make_async_remote_copy(
            src_ref=out_ref.at[to],
            dst_ref=in_ref.at[me],
            send_sem=sems.at[0],
            recv_sem=sems.at[1],
            device_id=place(to),
            device_id_type=MESH,
        )

    def pair(n, carry):
        send((me + n) % peers).start()
        send((me + peers - n) % peers).start()
        return carry

    def mate(n):
        to = (quarter + n) % QUARTERS
        return pltpu.make_async_remote_copy(
            src_ref=part_ref.at[to % part_ref.shape[0]],
            dst_ref=all_ref.at[quarter],
            send_sem=sems.at[2],
            recv_sem=sems.at[3],
            device_id=(ring, core, to),
            device_id_type=MESH,
        )

    send((me + peers // 2) % peers).start()
    for n in (2, 1, 3):
        mate(n).start()
    lax.fori_loop(1, peers // 2, pair, 0)
    swaps = []
    if swapping:
        swaps = [
            remote(src, dst, sems.at[6 + n], sems.at[9 + n], mate_core)
            for n, (src, dst) in enumerate(zip(weights, swapped))
        ]
        for copy in swaps:
            copy.start()
    for copy in own:
        copy.wait()
    some = slice(0, QUARTERS - 1)
    mates = pltpu.make_async_remote_copy(
        src_ref=all_ref.at[some],
        dst_ref=all_ref.at[some],
        send_sem=sems.at[2],
        recv_sem=sems.at[3],
        device_id=(ring, core, (quarter + 1) % QUARTERS),
        device_id_type=MESH,
    )
    most = slice(0, peers - 1)
    blocks = pltpu.make_async_remote_copy(
        src_ref=out_ref.at[most],
        dst_ref=in_ref.at[most],
        send_sem=sems.at[0],
        recv_sem=sems.at[1],
        device_id=place((me + 1) % peers),
        device_id_type=MESH,
    )
    for copy in (mates, blocks, *swaps):
        copy.wait_send()
        copy.wait_recv()


def exchange(blocks, part, name, number, swapped=()):
    rows = part.shape[1]
    return pl.pallas_call(
        exchange_kernel,
        in_specs=[pl.BlockSpec(memory_space=pltpu.VMEM)] * 2
        + [pl.BlockSpec(memory_space=pl.ANY)] * len(swapped),
        out_specs=[pl.BlockSpec(memory_space=pltpu.VMEM)] * 2
        + [pl.BlockSpec(memory_space=pl.ANY)] * len(swapped),
        out_shape=[sds(blocks.shape, BF16), sds((QUARTERS, rows, MODEL), BF16)]
        + [sds(w.shape, BF16) for w in swapped],
        scratch_shapes=[pltpu.SemaphoreType.DMA((12,))],
        compiler_params=pltpu.CompilerParams(collective_id=number, has_side_effects=True),
        cost_estimate=pl.CostEstimate(
            flops=15_000_000_000, bytes_accessed=4_000_000, transcendentals=0
        ),
        name=name,
    )(blocks, part, *swapped)


def per_device(
    head_queries,
    head_keys,
    head_values,
    decay_logits,
    learning_logits,
    surge_decay,
    documents,
    residual,
    head_norm_scale,
    mixer_output_weight,
    layer_norm_scale,
    routes,
    routing_weight,
    routed_gate_weight,
    routed_up_weight,
    routed_down_weight,
    common_gate_weight,
    common_up_weight,
    common_down_weight,
):
    rows = residual.shape[0]
    raw = (routed_gate_weight, routed_up_weight, routed_down_weight)
    near, stage, tail = mixer(
        head_queries,
        head_keys,
        head_values,
        decay_logits,
        learning_logits,
        surge_decay,
        documents,
        head_norm_scale,
        mixer_output_weight,
        (residual, layer_norm_scale, routes, routing_weight),
        raw,
    )
    stream, outgoing, pick, *moved = tail
    swap, zero, far = moved[:3], [w[None] for w in moved[3:6]], [w[None] for w in moved[6:]]
    slots = outgoing.shape[0]
    blocks = (slots // 2, 2, MODEL)
    incoming, rows_all, *far_swap = exchange(
        outgoing.reshape(blocks), stream[None], "dispatch", 1, far
    )
    shared_part = shared(
        rows_all.reshape(-1, MODEL), common_gate_weight, common_up_weight, common_down_weight
    )
    answers = expert(incoming.reshape(slots, MODEL), raw, (*stage, *zero, *near, *swap, *far, *far_swap))
    back, shared_rows = exchange(
        answers.reshape(blocks), shared_part.reshape(QUARTERS, rows, MODEL), "giveback", 2
    )
    return join(stream, back.reshape(slots, MODEL), pick, shared_rows)


def solution(mesh):
    torus = Mesh(mesh.devices.reshape(-1, 2, QUARTERS), ("ring", "core", "tp"))
    sp = ("ring", "core")
    rows = P(sp, "tp")
    own = P((*sp, "tp"), None)
    placed = (
        *(rows,) * 6,
        P(sp),
        own,
        P("tp"),
        P("tp", None),
        P(),
        P(sp, None),
        own,
        P(sp, None, "tp"),
        P(sp, None, "tp"),
        P(sp, "tp", None),
        P(None, "tp"),
        P(None, "tp"),
        P("tp", None),
    )
    return jax.shard_map(
        per_device, mesh=torus, in_specs=placed, out_specs=own, check_vma=False
    )
```
